128 devices in a mesh: rep: 2 (over z_hi), fs: 32 (over z_lo, y, x), tp: 2 (over core).
Axes of the slice: x: 4, y: 4, z: 4 (z_hi: 2, z_lo: 2; z = z_hi * 2 + z_lo), core: 2. Of those that a mesh axis runs over, the one named last changes fastest.
Arguments:
- tokens: bfloat16 [65536, 2048], P(('rep', 'fs'), 'tp'), may hold values from -6 to 6
- attention_pre_gain: float32 [2048], replicated, may hold values from 0.1 to 1.9
- query_matrix: bfloat16 [2048, 512], P('fs', 'tp'), may hold values from -0.125 to 0.125
- key_matrix: bfloat16 [2048, 512], P('fs', 'tp'), may hold values from -0.125 to 0.125
- value_matrix: bfloat16 [2048, 1024], P('fs', 'tp'), may hold values from -0.125 to 0.125
- decay_first_weight: bfloat16 [2048, 16], replicated, may hold values from -0.125 to 0.125
- decay_second_weight: bfloat16 [16, 512], P(None, 'tp'), may hold values from -1.5 to 1.5
- decay_offset_bias: float32 [512], P('tp'), may hold values from 0 to 6
- extra_log_surge: float32 [65536, 2], P(('rep', 'fs'), 'tp'), may hold values from -0.7 to 0
- readout_head_gain: float32 [512], replicated, may hold values from 0.1 to 1.9
- output_matrix: bfloat16 [1024, 2048], P('tp', 'fs'), may hold values from -2.4375 to 2.4375
- attention_post_gain: float32 [2048], P('tp'), may hold values from 0.1 to 1.9
- feedforward_pre_gain: float32 [2048], replicated, may hold values from 0.1 to 1.9
- up_matrix: bfloat16 [2048, 4096], P('fs', 'tp'), may hold values from -0.125 to 0.125
- down_matrix: bfloat16 [4096, 2048], P('tp', 'fs'), may hold values from -1.21875 to 1.21875
- feedforward_post_gain: float32 [2048], P('tp'), may hold values from 0.1 to 1.9
Outputs:
- layer_out: bfloat16 [65536, 2048], P(('rep', 'fs'), 'tp')
The draws below stay inside these ranges and needn't reach their ends.
All inputs are finite; a program needn't handle non-finite values.
Results may differ from the reference program's by a relative error of at most 0.017.
Values may be sent and summed in bfloat16 or wider, within the bound.
No kernel may reach another device: no remote copies, remote signals or barrier semaphores. Data moves between devices by JAX's collectives and lax.ppermute only.
A program may use at most 128 MiB of HBM per device.

```python
import jax
import jax.numpy as jnp
from jax import lax

D = 2048
FF = 4096
HEADS = 2
KEY_WIDTH = 256
DV = 512
RANK = 16
BLOCK = 64
LENGTH = 1024
KEYDIM = 512
VALDIM = 1024
TOKENS = 65536
N_TP = 2


def draw_decay_offset_bias(key, part):
    base = jax.random.fold_in(key, 11)
    first, second, third = jax.random.split(base, 3)
    slow_share = 0.5
    chosen = jax.random.uniform(first, (KEYDIM,), jnp.float32) < slow_share
    slow_value = jax.random.uniform(second, (KEYDIM,), jnp.float32, 4.0, 6.0)
    fast_value = jax.random.uniform(third, (KEYDIM,), jnp.float32, 0.0, 1.5)
    return jnp.where(chosen, slow_value, fast_value)


def draw_extra_log_surge(key, part):
    base = jax.random.fold_in(key, 23)
    first, second = jax.random.split(base, 2)
    marked = jax.random.randint(first, (TOKENS, HEADS), 0, LENGTH // 4) == 0
    sizes = jnp.log(jax.random.uniform(second, (TOKENS, HEADS), jnp.float32, 0.5, 0.8))
    return jnp.where(marked, sizes, jnp.zeros((TOKENS, HEADS), jnp.float32))


def ramped_matrix(key, rows, columns):
    first, second = jax.random.split(key, 2)
    entries = jnp.clip(jax.random.normal(first, (rows, columns), jnp.float32), -6.0, 6.0)
    top_scale = 10.0
    ramp = jnp.exp(jnp.log(top_scale) * jnp.arange(columns, dtype=jnp.float32) / columns)
    rough = jax.random.uniform(second, (columns,), jnp.float32, 0.7, 1.3)
    return (entries * rows ** (-0.5) * (ramp * rough)[None, :]).astype(jnp.bfloat16)


def draw_down_matrix(key, part):
    return ramped_matrix(jax.random.fold_in(key, 37), FF, D)


def draw_output_matrix(key, part):
    return ramped_matrix(jax.random.fold_in(key, 53), VALDIM, D)


def shard_levels(key, dims, pieces, low, high):
    factor_of, own = 1.0, jax.random.fold_in(key, 6)
    for position, parts in pieces:
        draws = jnp.exp(jax.random.uniform(jax.random.fold_in(own, position), (parts,), jnp.float32, low / len(pieces), high / len(pieces)))
        factor_of = factor_of * jnp.repeat(draws, dims[position] // parts).reshape([-1 if axis == position else 1 for axis in range(len(dims))])
    return factor_of


def bell_draw(stream_key, shape, deviation, limit, cuts=(), held_as=jnp.bfloat16):
    drawn = jax.random.normal(stream_key, shape, jnp.float32) * deviation
    if len(cuts) > 0:
        drawn = shard_levels(stream_key, shape, cuts, -0.22, 0.18) * drawn
    return jnp.clip(drawn, min=-limit, max=limit).astype(held_as)


def setup_inputs(seed: int = 0) -> dict:
    key_of = jax.random.split(jax.random.key(seed), 17)
    tokens = bell_draw(key_of[0], (TOKENS, D), 1.0, 6.0, ((0, 64), (1, 2)))
    attention_pre_gain = jnp.clip(1.0 + 0.18 * jax.random.normal(key_of[1], (D,), jnp.float32), 0.1, 1.9)
    query_matrix = bell_draw(key_of[2], (D, KEYDIM), D ** -0.5, 0.125, ((0, 32), (1, 2)))
    key_matrix = bell_draw(key_of[3], (D, KEYDIM), D ** -0.5, 0.125, ((0, 32), (1, 2)))
    value_matrix = bell_draw(key_of[4], (D, VALDIM), D ** -0.5, 0.125, ((0, 32), (1, 2)))
    decay_first_weight = bell_draw(key_of[5], (D, RANK), D ** -0.5, 0.125)
    decay_second_weight = bell_draw(key_of[6], (RANK, KEYDIM), RANK ** -0.5, 1.5, ((1, 2),))
    decay_offset_bias = draw_decay_offset_bias(jax.random.fold_in(key_of[16], 71), 0)
    extra_log_surge = draw_extra_log_surge(jax.random.fold_in(key_of[16], 71), 0)
    readout_head_gain = jnp.clip(1.0 + 0.18 * jax.random.normal(key_of[9], (DV,), jnp.float32), 0.1, 1.9)
    output_matrix = draw_output_matrix(jax.random.fold_in(key_of[16], 71), 0)
    attention_post_gain = jnp.clip(1.0 + 0.18 * jax.random.normal(key_of[11], (D,), jnp.float32), 0.1, 1.9)
    feedforward_pre_gain = jnp.clip(1.0 + 0.18 * jax.random.normal(key_of[12], (D,), jnp.float32), 0.1, 1.9)
    up_matrix = bell_draw(key_of[13], (D, FF), D ** -0.5, 0.125, ((0, 32), (1, 2)))
    down_matrix = draw_down_matrix(jax.random.fold_in(key_of[16], 71), 0)
    feedforward_post_gain = jnp.clip(1.0 + 0.18 * jax.random.normal(key_of[15], (D,), jnp.float32), 0.1, 1.9)
    return {"tokens": tokens, "attention_pre_gain": attention_pre_gain, "query_matrix": query_matrix, "key_matrix": key_matrix, "value_matrix": value_matrix, "decay_first_weight": decay_first_weight, "decay_second_weight": decay_second_weight, "decay_offset_bias": decay_offset_bias, "extra_log_surge": extra_log_surge, "readout_head_gain": readout_head_gain, "output_matrix": output_matrix, "attention_post_gain": attention_post_gain, "feedforward_pre_gain": feedforward_pre_gain, "up_matrix": up_matrix, "down_matrix": down_matrix, "feedforward_post_gain": feedforward_post_gain}


EPS = 1e-06

def pre_norm(rows, gain):
    values = rows.astype(jnp.float32)
    scale = lax.rsqrt(lax.optimization_barrier(jnp.mean(values * values, axis=-1, keepdims=True)) + EPS)
    return (values * scale * gain).astype(jnp.bfloat16)

def block_attention(queries, keys_in, values_in, log_gates):
    head_count, token_length, key_size = queries.shape
    value_size = values_in.shape[-1]
    blocks = token_length // BLOCK

    def to_blocks(array):
        return array.reshape(head_count, blocks, BLOCK, array.shape[-1]).transpose(1, 0, 2, 3)
    causal = jnp.tril(jnp.ones((BLOCK, BLOCK), dtype=bool))[None, :, :, None]
    highest = lax.Precision.HIGHEST

    def advance(memory_state, inputs):
        query_blk, key_blk, value_blk, gate_blk = inputs
        cumulative = jnp.cumsum(gate_blk, axis=1)
        carried = jnp.einsum('hid,hde->hie', query_blk * jnp.exp(cumulative), memory_state, precision=highest)
        spread_log = cumulative[:, :, None, :] - cumulative[:, None, :, :]
        weights = jnp.exp(jnp.where(causal, spread_log, -jnp.inf))
        scores = jnp.einsum('hid,hjd,hijd->hij', query_blk, key_blk, weights, precision=highest)
        readout = carried + jnp.einsum('hij,hje->hie', scores, value_blk, precision=highest)
        final_log = cumulative[:, -1:, :]
        memory_state = jnp.exp(final_log[:, 0, :])[:, :, None] * memory_state + jnp.einsum('hjd,hje->hde', key_blk * jnp.exp(final_log - cumulative), value_blk, precision=highest)
        return (memory_state, readout)
    start_state = jnp.zeros((head_count, key_size, value_size), jnp.float32)
    _, readout = lax.scan(advance, start_state, (to_blocks(queries), to_blocks(keys_in), to_blocks(values_in), to_blocks(log_gates)))
    return readout.transpose(1, 0, 2, 3).reshape(head_count, token_length, value_size)

def grouped_sum(left, right):
    group = left.shape[1] // N_TP
    total = jnp.zeros((left.shape[0], right.shape[1]), jnp.float32)
    for member in range(N_TP):
        partial_value = jnp.dot(left[:, member * group:(member + 1) * group], right[member * group:(member + 1) * group], preferred_element_type=jnp.float32)
        rounded = lax.optimization_barrier(partial_value.astype(jnp.bfloat16))
        total = total + rounded.astype(jnp.float32)
    return total

def post_add(resid, branch, gain):
    scale = lax.rsqrt(lax.optimization_barrier(jnp.mean(branch * branch, axis=-1, keepdims=True)) + EPS)
    return (resid.astype(jnp.float32) + branch * scale * gain).astype(jnp.bfloat16)

def reference(tokens, attention_pre_gain, query_matrix, key_matrix, value_matrix, decay_first_weight, decay_second_weight, decay_offset_bias, extra_log_surge, readout_head_gain, output_matrix, attention_post_gain, feedforward_pre_gain, up_matrix, down_matrix, feedforward_post_gain):
    normed = pre_norm(tokens, attention_pre_gain)
    query_proj = jnp.dot(normed, query_matrix, preferred_element_type=jnp.float32).astype(jnp.bfloat16)
    key_proj = jnp.dot(normed, key_matrix, preferred_element_type=jnp.float32).astype(jnp.bfloat16)
    value_proj = jnp.dot(normed, value_matrix, preferred_element_type=jnp.float32).astype(jnp.bfloat16)
    rank_rows = jnp.dot(normed, decay_first_weight, preferred_element_type=jnp.float32).astype(jnp.bfloat16)
    gate_source_input = jnp.dot(rank_rows, decay_second_weight, preferred_element_type=jnp.float32) + decay_offset_bias
    logarithm_decay = jax.nn.log_sigmoid(gate_source_input) / 16.0 + jnp.repeat(extra_log_surge, KEY_WIDTH, axis=1)
    sequences = TOKENS // LENGTH

    def by_head(array, size):
        return array.astype(jnp.float32).reshape(sequences, LENGTH, HEADS, size).transpose(0, 2, 1, 3)
    queries = by_head(query_proj, KEY_WIDTH) * KEY_WIDTH ** (-0.5)
    readout = lax.map(lambda group: block_attention(*group), (queries, by_head(key_proj, KEY_WIDTH), by_head(value_proj, DV), by_head(logarithm_decay, KEY_WIDTH)))
    readout = readout.transpose(0, 2, 1, 3).reshape(TOKENS, HEADS, DV)
    head_scale = lax.rsqrt(lax.optimization_barrier(jnp.mean(readout * readout, axis=-1, keepdims=True)) + EPS)
    mixed = (readout * head_scale * readout_head_gain).astype(jnp.bfloat16).reshape(TOKENS, VALDIM)
    attn = grouped_sum(mixed, output_matrix)
    resid = post_add(tokens, attn, attention_post_gain)
    normed_mid = pre_norm(resid, feedforward_pre_gain)
    hidden = jax.nn.relu(jnp.dot(normed_mid, up_matrix, preferred_element_type=jnp.float32))
    squared = (hidden * hidden).astype(jnp.bfloat16)
    feed = grouped_sum(squared, down_matrix)
    return post_add(resid, feed, feedforward_post_gain)
```

```python
import jax
import jax.numpy as jnp
import numpy as np
from jax import lax
from jax.experimental import pallas as pl
from jax.experimental.pallas import tpu as pltpu
from jax.sharding import Mesh
from jax.sharding import PartitionSpec as P

FS = ("fs_0", "fs_1", "fs_2")
REP_FS = ("rep", "fs_0", "fs_1", "fs_2")
ALL = ("rep", "fs_0", "fs_1", "fs_2", "tp")
EPS = 1e-06
CHUNK = 256
HALF = 32
BF = jnp.bfloat16
F32 = jnp.float32


CLASSES = (("x", 1), ("y", 1), ("z", 1), ("x", 3), ("y", 3), ("z", 3))


def link_class(step, chain, core):
    return CLASSES[(step + 2 * chain + core) % 6]


def partner_pairs(step, chain):
    pairs = []
    for z in range(4):
        for y in range(4):
            for x in range(4):
                for core in range(2):
                    axis, flip = link_class(step, chain, core)
                    to = {"x": x, "y": y, "z": z}
                    to[axis] ^= flip
                    source = ((z * 4 + y) * 4 + x) * 2 + core
                    target = ((to["z"] * 4 + to["y"]) * 4 + to["x"]) * 2 + core
                    pairs.append((source, target))
    return pairs


def row_block(z, y, x):
    return (((z & 1) * 16 + y * 4 + x) << 1) | (z >> 1)


def block_offsets():
    table = np.zeros((2, 3, 64), np.int32)
    for core in range(2):
        for chain in range(3):
            for place in range(64):
                total = 0
                for step in range(6):
                    if place >> step & 1:
                        axis, flip = link_class(step, chain, core)
                        at = {"x": 0, "y": 0, "z": 0}
                        at[axis] = flip
                        total ^= row_block(at["z"], at["y"], at["x"])
                table[core, chain, place] = total
    return table


OFFSETS = block_offsets()


def swap_cores(array):
    return lax.ppermute(array, "tp", [(0, 1), (1, 0)])


def gather_chain(own, chain, split_last):
    held = own
    for step in range(4):
        came = lax.ppermute(held, ALL, partner_pairs(step, chain))
        held = jnp.concatenate([held, came], axis=0)
    came = lax.ppermute(held, ALL, partner_pairs(4, chain))
    if split_last:
        last = partner_pairs(5, chain)
        return [held, came, lax.ppermute(held, ALL, last), lax.ppermute(came, ALL, last)]
    held = jnp.concatenate([held, came], axis=0)
    return [held, lax.ppermute(held, ALL, partner_pairs(5, chain))]


def start_pieces(table, pieces, chain, lanes, target, target_lane, sem):
    place = 0
    for piece in pieces:
        count = piece.shape[0] // HALF

        def one(i, carry, piece=piece, place=place):
            block = table[chain, place + i]
            pltpu.make_async_copy(
                piece.at[pl.ds(pl.multiple_of(i * HALF, HALF), HALF), pl.ds(lanes[0], lanes[1])],
                target.at[
                    pl.ds(pl.multiple_of(block * HALF, HALF), HALF), pl.ds(target_lane, lanes[1])
                ],
                sem,
            ).start()
            return carry

        lax.fori_loop(0, count, one, 0)
        place += count


def wait_part(target, lane, width, sem):
    part = target.at[:, pl.ds(lane, width)]
    pltpu.make_async_copy(part, part, sem).wait()


def nt_dot(a, b):
    return lax.dot_general(a, b, (((1,), (1,)), ((), ())), preferred_element_type=F32)


def tn_dot(a, b):
    return lax.dot_general(a, b, (((0,), (0,)), ((), ())), preferred_element_type=F32)


def ordered(core, own, other):
    first = core == 0
    return jnp.concatenate([jnp.where(first, own, other), jnp.where(first, other, own)], axis=1)


def norm_kernel(core, own, other, gain, first, second, bias, surge, normed_out, decay_out):
    rows = ordered(core[0], own[...], other[...]).astype(F32)
    scale = lax.rsqrt(jnp.mean(rows * rows, axis=-1, keepdims=True) + EPS)
    normed = (rows * scale * gain[...]).astype(BF)
    normed_out[...] = normed
    rank = jnp.dot(normed, first[...], preferred_element_type=F32).astype(BF)
    gate = jnp.dot(rank, second[...], preferred_element_type=F32) + bias[...]
    decay_out[...] = jax.nn.log_sigmoid(gate) / 16.0 + surge[...]


def level_matrices():
    i = np.arange(CHUNK)[:, None]
    t = np.arange(CHUNK)[None, :]
    mats = []
    size = 1
    while size < CHUNK:
        same = i // (2 * size) == t // (2 * size)
        upper_i, upper_t = i % (2 * size) >= size, t % (2 * size) >= size
        mats.append(same & ((upper_i & upper_t & (t <= i)) | (~upper_i & ~upper_t & (t > i))))
        size *= 2
    mats.append(t <= i)
    mats.append(t > i)
    return np.concatenate(mats, axis=0)


LEVELS = level_matrices()
N_LEVELS = 8


def attention_kernel(
    table, normed, decay, levels, gain, *rest
):
    qk_pieces, v_pieces = rest[0:2], rest[2:4]
    mixed_out, w_qk, w_v, state, sems = rest[4:]
    step = pl.program_id(0)

    @pl.when(step == 0)
    def _():
        start_pieces(table, qk_pieces, 0, (0, 512), w_qk, 0, sems.at[0])
        start_pieces(table, v_pieces, 1, (0, 512), w_v, 0, sems.at[1])
        state[...] = jnp.zeros_like(state)
        wait_part(w_qk, 0, 512, sems.at[0])
        wait_part(w_v, 0, 512, sems.at[1])

    rows = normed[...]
    qk = jnp.dot(rows, w_qk[...], preferred_element_type=F32).astype(BF).astype(F32)
    q, k = qk[:, :256] * (256**-0.5), qk[:, 256:]
    v = jnp.dot(rows, w_v[...], preferred_element_type=F32).astype(BF)

    g = decay[...]
    g_hi = g.astype(BF)
    g_lo = (g - g_hi.astype(F32)).astype(BF)

    def exponent(level):
        mat = levels[pl.ds(level * CHUNK, CHUNK), :]
        return jnp.dot(mat, g_hi, preferred_element_type=F32) + jnp.dot(
            mat, g_lo, preferred_element_type=F32
        )

    row = lax.broadcasted_iota(jnp.int32, (CHUNK, CHUNK), 0)
    col = lax.broadcasted_iota(jnp.int32, (CHUNK, CHUNK), 1)
    scores = jnp.zeros((CHUNK, CHUNK), F32)
    for level in range(N_LEVELS):
        size = 1 << level
        upper = (row & size) != 0
        both = (jnp.where(upper, q, k) * jnp.exp(exponent(level))).astype(BF)
        pair = upper & ((col & size) == 0) & ((row >> (level + 1)) == (col >> (level + 1)))
        scores = jnp.where(pair, nt_dot(both, both), scores)
    to_here = exponent(N_LEVELS)
    to_end = exponent(N_LEVELS + 1)
    q_in = (q * jnp.exp(to_here)).astype(BF)
    k_out = (k * jnp.exp(to_end)).astype(BF)
    old = state[...]
    readout = (
        nt_dot(q_in, old.astype(BF))
        + jnp.dot(scores.astype(BF), v, preferred_element_type=F32)
        + jnp.sum(q * k, axis=1, keepdims=True) * v.astype(F32)
    )
    state[...] = old * jnp.exp(to_here[CHUNK - 1 :, :]) + tn_dot(v, k_out)
    scale = lax.rsqrt(jnp.mean(readout * readout, axis=-1, keepdims=True) + EPS)
    mixed_out[...] = (readout * scale * gain[...]).astype(BF)


def out_kernel(table, mixed, *rest):
    pieces = rest[0:2]
    partial_out, weight, sems = rest[2:]

    @pl.when(pl.program_id(0) == 0)
    def _():
        start_pieces(table, pieces, 2, (0, 512), weight, 0, sems.at[0])
        wait_part(weight, 0, 512, sems.at[0])

    partial_out[...] = nt_dot(mixed[...], weight[...]).astype(BF)


UP_WIDTHS = (768, 640, 640)
DOWN_WIDTHS = (640, 640, 768)


def start_of(widths, chain):
    return sum(widths[:chain])


def up_kernel(
    core, table, own, other, mine, theirs, post_gain, pre_gain, *rest
):
    pieces = [rest[4 * c : 4 * c + 4] for c in range(3)]
    resid_out, squared_out, weight, sems = rest[12:]
    first_step = pl.program_id(0) == 0

    @pl.when(first_step)
    def _():
        for c in range(3):
            start_pieces(
                table, pieces[c], c, (0, UP_WIDTHS[c]), weight, start_of(UP_WIDTHS, c), sems.at[c]
            )

    rows = ordered(core[0], own[...], other[...]).astype(F32)
    attn = mine[...].astype(F32) + theirs[...].astype(F32)
    scale = lax.rsqrt(jnp.mean(attn * attn, axis=-1, keepdims=True) + EPS)
    resid = (rows + attn * scale * post_gain[...]).astype(BF)
    resid_out[...] = resid
    values = resid.astype(F32)
    scale = lax.rsqrt(jnp.mean(values * values, axis=-1, keepdims=True) + EPS)
    normed = (values * scale * pre_gain[...]).astype(BF)
    for c in range(3):
        at, width = start_of(UP_WIDTHS, c), UP_WIDTHS[c]

        @pl.when(first_step)
        def _(at=at, width=width, c=c):
            wait_part(weight, at, width, sems.at[c])

        hidden = jnp.dot(normed, weight[:, at : at + width], preferred_element_type=F32)
        hidden = jnp.maximum(hidden, 0.0)
        squared_out[:, at : at + width] = (hidden * hidden).astype(BF)


def down_kernel(table, squared, *rest):
    pieces = [rest[4 * c : 4 * c + 4] for c in range(3)]
    partial_out, weight, sems = rest[12:]

    @pl.when(pl.program_id(0) == 0)
    def _():
        for c in range(3):
            at, width = start_of(DOWN_WIDTHS, c), DOWN_WIDTHS[c]
            start_pieces(table, pieces[c], c, (UP_WIDTHS[c], width), weight, at, sems.at[c])
        for c in range(3):
            wait_part(weight, start_of(DOWN_WIDTHS, c), DOWN_WIDTHS[c], sems.at[c])

    partial_out[...] = nt_dot(squared[...], weight[...]).astype(BF)


def final_kernel(core, resid, mine, theirs, gain, out):
    feed = mine[...].astype(F32) + theirs[...].astype(F32)
    scale = lax.rsqrt(jnp.mean(feed * feed, axis=-1, keepdims=True) + EPS)
    low = core[0] == 0
    feed_own = jnp.where(low, feed[:, :1024], feed[:, 1024:])
    resid_all = resid[...]
    resid_own = jnp.where(low, resid_all[:, :1024], resid_all[:, 1024:])
    out[...] = (resid_own.astype(F32) + feed_own * scale * gain[...]).astype(BF)


SMEM = pl.BlockSpec(memory_space=pltpu.SMEM)
HBM = pl.BlockSpec(memory_space=pltpu.HBM)


def whole(shape):
    return pl.BlockSpec(shape, lambda i: (0,) * len(shape))


def rows_of(count, width):
    return pl.BlockSpec((count, width), lambda i: (i, 0))


def params(flops, nbytes):
    return dict(
        compiler_params=pltpu.CompilerParams(
            dimension_semantics=("arbitrary",), vmem_limit_bytes=58 * 1024 * 1024
        ),
        cost_estimate=pl.CostEstimate(flops=flops, bytes_accessed=nbytes, transcendentals=0),
    )


def on_device(
    tokens,
    attention_pre_gain,
    query_matrix,
    key_matrix,
    value_matrix,
    decay_first_weight,
    decay_second_weight,
    decay_offset_bias,
    extra_log_surge,
    readout_head_gain,
    output_matrix,
    attention_post_gain,
    feedforward_pre_gain,
    up_matrix,
    down_matrix,
    feedforward_post_gain,
):
    length = tokens.shape[0]
    rep, core = lax.axis_index("rep"), lax.axis_index("tp")
    fs = lax.axis_index(FS)
    mine = fs * 2 + rep
    core_in = core.astype(jnp.int32).reshape(1)
    table = jnp.asarray(OFFSETS)[core] ^ mine.astype(jnp.int32)

    def half(shard):
        return lax.dynamic_slice_in_dim(shard, rep * HALF, HALF, axis=0)

    qk = gather_chain(jnp.concatenate([half(query_matrix), half(key_matrix)], axis=1), 0, False)
    v = gather_chain(half(value_matrix), 1, False)
    out_w = gather_chain(half(output_matrix.T), 2, False)
    up, down = half(up_matrix), half(down_matrix.T)
    feed_w = []
    for c in range(3):
        a, b = start_of(UP_WIDTHS, c), start_of(DOWN_WIDTHS, c)
        both = jnp.concatenate(
            [up[:, a : a + UP_WIDTHS[c]], down[:, b : b + DOWN_WIDTHS[c]]], axis=1
        )
        feed_w += gather_chain(both, c, True)

    other = swap_cores(tokens)
    block = 256
    grid = (length // block,)
    normed, decay = pl.pallas_call(
        norm_kernel,
        grid=grid,
        in_specs=[
            SMEM,
            rows_of(block, 1024),
            rows_of(block, 1024),
            whole((1, 2048)),
            whole((2048, 16)),
            whole((16, 256)),
            whole((1, 256)),
            rows_of(block, 1),
        ],
        out_specs=[rows_of(block, 2048), rows_of(block, 256)],
        out_shape=[
            jax.ShapeDtypeStruct((length, 2048), BF),
            jax.ShapeDtypeStruct((length, 256), F32),
        ],
        name="norm",
        **params(400_000_000, 10_000_000),
    )(
        core_in,
        tokens,
        other,
        attention_pre_gain.reshape(1, -1),
        decay_first_weight,
        decay_second_weight,
        decay_offset_bias.reshape(1, -1),
        extra_log_surge,
    )
    mixed = pl.pallas_call(
        attention_kernel,
        grid=(length // CHUNK,),
        in_specs=[
            SMEM,
            rows_of(CHUNK, 2048),
            rows_of(CHUNK, 256),
            whole(LEVELS.shape),
            whole((1, 512)),
        ]
        + [HBM] * 4,
        out_specs=rows_of(CHUNK, 512),
        out_shape=jax.ShapeDtypeStruct((length, 512), BF),
        scratch_shapes=[
            pltpu.VMEM((2048, 512), BF),
            pltpu.VMEM((2048, 512), BF),
            pltpu.VMEM((512, 256), F32),
            pltpu.SemaphoreType.DMA((2,)),
        ],
        name="attention",
        **params(9_000_000_000, 14_000_000),
    )(
        table,
        normed,
        decay,
        jnp.asarray(LEVELS, BF),
        readout_head_gain.reshape(1, -1),
        *qk,
        *v,
    )
    partial_attn = pl.pallas_call(
        out_kernel,
        grid=grid,
        in_specs=[SMEM, rows_of(block, 512)] + [HBM] * 2,
        out_specs=rows_of(block, 2048),
        out_shape=jax.ShapeDtypeStruct((length, 2048), BF),
        scratch_shapes=[pltpu.VMEM((2048, 512), BF), pltpu.SemaphoreType.DMA((1,))],
        name="out_proj",
        **params(2_200_000_000, 8_000_000),
    )(table, mixed, *out_w)
    other_attn = swap_cores(partial_attn)
    post_gain = lax.all_gather(attention_post_gain, "tp", tiled=True).reshape(1, -1)
    resid, squared = pl.pallas_call(
        up_kernel,
        grid=grid,
        in_specs=[
            SMEM,
            SMEM,
            rows_of(block, 1024),
            rows_of(block, 1024),
            rows_of(block, 2048),
            rows_of(block, 2048),
            whole((1, 2048)),
            whole((1, 2048)),
        ]
        + [HBM] * 12,
        out_specs=[rows_of(block, 2048), rows_of(block, 2048)],
        out_shape=[
            jax.ShapeDtypeStruct((length, 2048), BF),
            jax.ShapeDtypeStruct((length, 2048), BF),
        ],
        scratch_shapes=[pltpu.VMEM((2048, 2048), BF), pltpu.SemaphoreType.DMA((3,))],
        name="up_proj",
        **params(8_700_000_000, 28_000_000),
    )(
        core_in,
        table,
        tokens,
        other,
        partial_attn,
        other_attn,
        post_gain,
        feedforward_pre_gain.reshape(1, -1),
        *feed_w,
    )
    partial_feed = pl.pallas_call(
        down_kernel,
        grid=grid,
        in_specs=[SMEM, rows_of(block, 2048)] + [HBM] * 12,
        out_specs=rows_of(block, 2048),
        out_shape=jax.ShapeDtypeStruct((length, 2048), BF),
        scratch_shapes=[pltpu.VMEM((2048, 2048), BF), pltpu.SemaphoreType.DMA((3,))],
        name="down_proj",
        **params(8_700_000_000, 16_000_000),
    )(table, squared, *feed_w)
    other_feed = swap_cores(partial_feed)
    return pl.pallas_call(
        final_kernel,
        grid=grid,
        in_specs=[
            SMEM,
            rows_of(block, 2048),
            rows_of(block, 2048),
            rows_of(block, 2048),
            whole((1, 1024)),
        ],
        out_specs=rows_of(block, 1024),
        out_shape=jax.ShapeDtypeStruct((length, 1024), BF),
        name="final",
        **params(20_000_000, 14_000_000),
    )(core_in, resid, partial_feed, other_feed, feedforward_post_gain.reshape(1, -1))


def solution(mesh):
    finer = Mesh(
        mesh.devices.reshape(mesh.shape["rep"], 2, 4, 4, mesh.shape["tp"]),
        ("rep", "fs_0", "fs_1", "fs_2", "tp"),
    )
    in_specs = (
        P(REP_FS, "tp"),
        P(),
        P(FS, "tp"),
        P(FS, "tp"),
        P(FS, "tp"),
        P(),
        P(None, "tp"),
        P("tp"),
        P(REP_FS, "tp"),
        P(),
        P("tp", FS),
        P("tp"),
        P(),
        P(FS, "tp"),
        P("tp", FS),
        P("tp"),
    )
    return jax.shard_map(
        on_device, mesh=finer, in_specs=in_specs, out_specs=P(REP_FS, "tp"), check_vma=False
    )
```

```python
import jax
import jax.numpy as jnp
import numpy as np
from jax import lax
from jax.experimental import pallas as pl
from jax.experimental.pallas import tpu as pltpu
from jax.sharding import Mesh
from jax.sharding import PartitionSpec as P


FS = ("fs_0", "fs_1", "fs_2")
REP_FS = ("rep", "fs_0", "fs_1", "fs_2")
ALL = ("rep", "fs_0", "fs_1", "fs_2", "tp")
EPS = 1e-06
CHUNK = 256
HALF = 32
BF = jnp.bfloat16
F32 = jnp.float32


CLASSES = (("x", 1), ("y", 1), ("z", 1), ("x", 3), ("y", 3), ("z", 3))


def link_class(step, chain, core):
    return CLASSES[(step + 2 * chain + core) % 6]


def partner_pairs(step, chain):
    pairs = []
    for z in range(4):
        for y in range(4):
            for x in range(4):
                for core in range(2):
                    axis, flip = link_class(step, chain, core)
                    to = {"x": x, "y": y, "z": z}
                    to[axis] ^= flip
                    source = ((z * 4 + y) * 4 + x) * 2 + core
                    target = ((to["z"] * 4 + to["y"]) * 4 + to["x"]) * 2 + core
                    pairs.append((source, target))
    return pairs


def row_block(z, y, x):
    return (((z & 1) * 16 + y * 4 + x) << 1) | (z >> 1)


def block_offsets():
    table = np.zeros((2, 3, 64), np.int32)
    for core in range(2):
        for chain in range(3):
            for place in range(64):
                total = 0
                for step in range(6):
                    if place >> step & 1:
                        axis, flip = link_class(step, chain, core)
                        at = {"x": 0, "y": 0, "z": 0}
                        at[axis] = flip
                        total ^= row_block(at["z"], at["y"], at["x"])
                table[core, chain, place] = total
    return table


OFFSETS = block_offsets()


def swap_cores(array):
    return lax.ppermute(array, "tp", [(0, 1), (1, 0)])


def over_link(array, step, chain):
    return lax.ppermute(array, ALL, partner_pairs(step, chain))


def stacked(a, b, lane, width):
    return jnp.concatenate([a[:, lane : lane + width], b[:, lane : lane + width]], axis=0)


MERGED_STEPS = 3


def gather_chain(first, up, down, chain):
    widths = (first.shape[1], up.shape[1], down.shape[1])
    held = jnp.concatenate([first, up, down], axis=1)
    for step in range(MERGED_STEPS):
        came = over_link(held, step, chain)
        if step < MERGED_STEPS - 1:
            held = jnp.concatenate([held, came], axis=0)
    first = stacked(held, came, 0, widths[0])
    feed = stacked(held, came, widths[0], widths[1] + widths[2])
    for step in range(MERGED_STEPS, 5):
        first = jnp.concatenate([first, over_link(first, step, chain)], axis=0)
    first = [first, over_link(first, 5, chain)]
    for step in range(MERGED_STEPS, 5):
        came = over_link(feed, step, chain)
        if step < 4:
            feed = jnp.concatenate([feed, came], axis=0)
    up = stacked(feed, came, 0, widths[1])
    down = stacked(feed, came, widths[1], widths[2])
    up = [up, over_link(up, 5, chain)]
    down = [down, over_link(down, 5, chain)]
    return first, up, down


def start_pieces(table, pieces, chain, lanes, target, target_lane, sem, first_block=None):
    place = 0
    for piece in pieces:
        count = piece.shape[0] // HALF

        def one(i, carry, piece=piece, place=place):
            block = table[chain, place + i]

            def copy(to):
                pltpu.make_async_copy(
                    piece.at[pl.ds(pl.multiple_of(i * HALF, HALF), HALF), pl.ds(*lanes)],
                    target.at[
                        pl.ds(pl.multiple_of(to * HALF, HALF), HALF), pl.ds(target_lane, lanes[1])
                    ],
                    sem,
                ).start()

            if first_block is None:
                copy(block)
            else:
                to = block - first_block
                pl.when((to >= 0) & (to < 32))(lambda: copy(to))
            return carry

        lax.fori_loop(0, count, one, 0, unroll=8)
        place += count


def wait_part(target, lane, width, sem):
    part = target.at[:, pl.ds(lane, width)]
    pltpu.make_async_copy(part, part, sem).wait()


def nt_dot(a, b):
    return lax.dot_general(a, b, (((1,), (1,)), ((), ())), preferred_element_type=F32)


def tn_dot(a, b):
    return lax.dot_general(a, b, (((0,), (0,)), ((), ())), preferred_element_type=F32)


def ordered(core, own, other):
    first = core == 0
    return jnp.concatenate([jnp.where(first, own, other), jnp.where(first, other, own)], axis=1)


def norm_kernel(core, own, other, gain, first, second, bias, surge, normed_out, decay_out):
    rows = ordered(core[0], own[...], other[...]).astype(F32)
    scale = lax.rsqrt(jnp.mean(rows * rows, axis=-1, keepdims=True) + EPS)
    normed = (rows * scale * gain[...]).astype(BF)
    normed_out[...] = normed
    rank = jnp.dot(normed, first[...], preferred_element_type=F32).astype(BF)
    gate = jnp.dot(rank, second[...], preferred_element_type=F32) + bias[...]
    decay_out[...] = jax.nn.log_sigmoid(gate) / 16.0 + surge[...]


def small_level_matrices():
    i = np.arange(CHUNK)[:, None]
    t = np.arange(CHUNK)[None, :]
    mats = []
    for size in (2, 4):
        same = i // (2 * size) == t // (2 * size)
        upper_i, upper_t = i % (2 * size) >= size, t % (2 * size) >= size
        mats.append(same & ((upper_i & upper_t & (t <= i)) | (~upper_i & ~upper_t & (t > i))))
    same = i // 8 == t // 8
    mats.append(same & (t <= i))
    mats.append(same & (t > i))
    return np.concatenate(mats, axis=0)


def level_of_pairs():
    i = np.arange(CHUNK)[:, None]
    j = np.arange(CHUNK)[None, :]
    level = np.floor(np.log2(np.maximum(i ^ j, 1))).astype(np.int32)
    return np.where(j < i, level, -1).astype(np.int32)


SMALL_LEVELS = small_level_matrices()
PAIR_LEVELS = level_of_pairs()


def attention_kernel(table, normed, decay, mats, pair_level, gain, *rest):
    pieces = (rest[0:2], rest[2:4], rest[4:6])
    partial_out, w_qk, w_v, w_out, state, sems = rest[6:]
    weights = (w_qk, w_v, w_out)
    first_step = pl.program_id(0) == 0

    @pl.when(first_step)
    def _():
        for c in range(3):
            start_pieces(table, pieces[c], c, (0, 512), weights[c], 0, sems.at[c])
        state[...] = jnp.zeros_like(state)

    g = decay[...]
    g_hi = g.astype(BF)
    g_lo = (g - g_hi.astype(F32)).astype(BF)

    def summed(index):
        mat = mats[pl.ds(index * CHUNK, CHUNK), :]
        return jnp.dot(mat, g_hi, preferred_element_type=F32) + jnp.dot(
            mat, g_lo, preferred_element_type=F32
        )

    before, after = summed(2), summed(3)
    row = lax.broadcasted_iota(jnp.int32, (CHUNK, CHUNK), 0)
    spans = [jnp.where((row & 1) != 0, g, 0.0), summed(0), summed(1)]
    size = 8
    while size < CHUNK:
        b = before.reshape(CHUNK // (2 * size), 2, size, CHUNK)
        a = after.reshape(CHUNK // (2 * size), 2, size, CHUNK)
        spans.append(jnp.stack([a[:, 0], b[:, 1]], axis=1).reshape(CHUNK, CHUNK))
        low, high = b[:, 0, size - 1 :, :], b[:, 1, size - 1 :, :]
        before = jnp.stack([b[:, 0], b[:, 1] + low], axis=1).reshape(CHUNK, CHUNK)
        after = jnp.stack([a[:, 0] + high, a[:, 1]], axis=1).reshape(CHUNK, CHUNK)
        size *= 2

    @pl.when(first_step)
    def _():
        for c in range(3):
            wait_part(weights[c], 0, 512, sems.at[c])

    rows = normed[...]
    qk = jnp.dot(rows, w_qk[...], preferred_element_type=F32).astype(BF).astype(F32)
    q, k = qk[:, :256] * (256**-0.5), qk[:, 256:]
    v = jnp.dot(rows, w_v[...], preferred_element_type=F32).astype(BF)
    level_map = pair_level[...]
    scores = jnp.zeros((CHUNK, CHUNK), F32)
    for level, span in enumerate(spans):
        both = (jnp.where((row & (1 << level)) != 0, q, k) * jnp.exp(span)).astype(BF)
        scores = jnp.where(level_map == level, nt_dot(both, both), scores)
    q_in = (q * jnp.exp(before)).astype(BF)
    k_out = (k * jnp.exp(after)).astype(BF)
    old = state[...]
    readout = (
        nt_dot(q_in, old.astype(BF))
        + jnp.dot(scores.astype(BF), v, preferred_element_type=F32)
        + jnp.sum(q * k, axis=1, keepdims=True) * v.astype(F32)
    )
    state[...] = old * jnp.exp(before[CHUNK - 1 :, :]) + tn_dot(v, k_out)
    scale = lax.rsqrt(jnp.mean(readout * readout, axis=-1, keepdims=True) + EPS)
    mixed = (readout * scale * gain[...]).astype(BF)
    partial_out[...] = nt_dot(mixed, w_out[...]).astype(BF)


UP_WIDTHS = (768, 640, 640)
DOWN_WIDTHS = (640, 640, 768)


def start_of(widths, chain):
    return sum(widths[:chain])


def up_kernel(
    core, table, own, other, mine, theirs, post_gain, pre_gain, *rest
):
    pieces = [rest[2 * c : 2 * c + 2] for c in range(3)]
    resid_out, squared_out, weight, sems = rest[6:]
    first_step = pl.program_id(0) == 0

    @pl.when(first_step)
    def _():
        for c in range(3):
            start_pieces(
                table, pieces[c], c, (0, UP_WIDTHS[c]), weight, start_of(UP_WIDTHS, c), sems.at[c]
            )

    rows = ordered(core[0], own[...], other[...]).astype(F32)
    attn = mine[...].astype(F32) + theirs[...].astype(F32)
    scale = lax.rsqrt(jnp.mean(attn * attn, axis=-1, keepdims=True) + EPS)
    resid = (rows + attn * scale * post_gain[...]).astype(BF)
    resid_out[...] = resid
    values = resid.astype(F32)
    scale = lax.rsqrt(jnp.mean(values * values, axis=-1, keepdims=True) + EPS)
    normed = (values * scale * pre_gain[...]).astype(BF)
    for c in range(3):
        at, width = start_of(UP_WIDTHS, c), UP_WIDTHS[c]

        @pl.when(first_step)
        def _(at=at, width=width, c=c):
            wait_part(weight, at, width, sems.at[c])

        hidden = jnp.dot(normed, weight[:, at : at + width], preferred_element_type=F32)
        hidden = jnp.maximum(hidden, 0.0)
        squared_out[:, at : at + width] = (hidden * hidden).astype(BF)


def down_kernel(table, side, squared, *rest):
    pieces = [rest[2 * c : 2 * c + 2] for c in range(3)]
    partial_out, weight, sems = rest[6:]

    @pl.when(pl.program_id(0) == 0)
    def _():
        for c in range(3):
            at, width = start_of(DOWN_WIDTHS, c), DOWN_WIDTHS[c]
            start_pieces(
                table, pieces[c], c, (0, width), weight, at, sems.at[c], side[0] * 32
            )
        for c in range(3):
            wait_part(weight, start_of(DOWN_WIDTHS, c), DOWN_WIDTHS[c], sems.at[c])

    partial_out[...] = nt_dot(squared[...], weight[...]).astype(BF)


SMEM = pl.BlockSpec(memory_space=pltpu.SMEM)
HBM = pl.BlockSpec(memory_space=pltpu.HBM)


def whole(shape):
    return pl.BlockSpec(shape, lambda i: (0,) * len(shape))


def rows_of(count, width):
    return pl.BlockSpec((count, width), lambda i: (i, 0))


def params(flops, nbytes, vmem_mib):
    return dict(
        compiler_params=pltpu.CompilerParams(
            dimension_semantics=("arbitrary",), vmem_limit_bytes=vmem_mib * 1024 * 1024
        ),
        cost_estimate=pl.CostEstimate(flops=flops, bytes_accessed=nbytes, transcendentals=0),
    )


def on_device(
    tokens,
    attention_pre_gain,
    query_matrix,
    key_matrix,
    value_matrix,
    decay_first_weight,
    decay_second_weight,
    decay_offset_bias,
    extra_log_surge,
    readout_head_gain,
    output_matrix,
    attention_post_gain,
    feedforward_pre_gain,
    up_matrix,
    down_matrix,
    feedforward_post_gain,
):
    length = tokens.shape[0]
    rep, core = lax.axis_index("rep"), lax.axis_index("tp")
    fs = lax.axis_index(FS)
    mine = fs * 2 + rep
    core_in = core.astype(jnp.int32).reshape(1)
    table = jnp.asarray(OFFSETS)[core] ^ mine.astype(jnp.int32)

    def half(shard):
        return lax.dynamic_slice_in_dim(shard, rep * HALF, HALF, axis=0)

    firsts = (
        jnp.concatenate([half(query_matrix), half(key_matrix)], axis=1),
        half(value_matrix),
        half(output_matrix.T),
    )
    up, down = half(up_matrix), half(down_matrix.T)
    gathered = []
    for c in range(3):
        a, b = start_of(UP_WIDTHS, c), start_of(DOWN_WIDTHS, c)
        gathered.append(
            gather_chain(
                firsts[c], up[:, a : a + UP_WIDTHS[c]], down[:, b : b + DOWN_WIDTHS[c]], c
            )
        )
    (qk, up_0, down_0), (v, up_1, down_1), (out_w, up_2, down_2) = gathered
    up_w = [*up_0, *up_1, *up_2]
    down_w = [*down_0, *down_1, *down_2]

    other = swap_cores(tokens)
    block = 256
    grid = (length // block,)
    normed, decay = pl.pallas_call(
        norm_kernel,
        grid=grid,
        in_specs=[
            SMEM,
            rows_of(block, 1024),
            rows_of(block, 1024),
            whole((1, 2048)),
            whole((2048, 16)),
            whole((16, 256)),
            whole((1, 256)),
            rows_of(block, 1),
        ],
        out_specs=[rows_of(block, 2048), rows_of(block, 256)],
        out_shape=[
            jax.ShapeDtypeStruct((length, 2048), BF),
            jax.ShapeDtypeStruct((length, 256), F32),
        ],
        name="norm",
        **params(400_000_000, 10_000_000, 16),
    )(
        core_in,
        tokens,
        other,
        attention_pre_gain.reshape(1, -1),
        decay_first_weight,
        decay_second_weight,
        decay_offset_bias.reshape(1, -1),
        extra_log_surge,
    )
    partial_attn = pl.pallas_call(
        attention_kernel,
        grid=(length // CHUNK,),
        in_specs=[
            SMEM,
            rows_of(CHUNK, 2048),
            rows_of(CHUNK, 256),
            whole(SMALL_LEVELS.shape),
            whole(PAIR_LEVELS.shape),
            whole((1, 512)),
        ]
        + [HBM] * 6,
        out_specs=rows_of(CHUNK, 2048),
        out_shape=jax.ShapeDtypeStruct((length, 2048), BF),
        scratch_shapes=[
            pltpu.VMEM((2048, 512), BF),
            pltpu.VMEM((2048, 512), BF),
            pltpu.VMEM((2048, 512), BF),
            pltpu.VMEM((512, 256), F32),
            pltpu.SemaphoreType.DMA((3,)),
        ],
        name="attention",
        **params(11_000_000_000, 14_000_000, 28),
    )(
        table,
        normed,
        decay,
        jnp.asarray(SMALL_LEVELS, BF),
        jnp.asarray(PAIR_LEVELS),
        readout_head_gain.reshape(1, -1),
        *qk,
        *v,
        *out_w,
    )
    other_attn = swap_cores(partial_attn)
    post_gain = lax.all_gather(attention_post_gain, "tp", tiled=True).reshape(1, -1)
    resid, squared = pl.pallas_call(
        up_kernel,
        grid=grid,
        in_specs=[
            SMEM,
            SMEM,
            rows_of(block, 1024),
            rows_of(block, 1024),
            rows_of(block, 2048),
            rows_of(block, 2048),
            whole((1, 2048)),
            whole((1, 2048)),
        ]
        + [HBM] * 6,
        out_specs=[rows_of(block, 2048), rows_of(block, 2048)],
        out_shape=[
            jax.ShapeDtypeStruct((length, 2048), BF),
            jax.ShapeDtypeStruct((length, 2048), BF),
        ],
        scratch_shapes=[pltpu.VMEM((2048, 2048), BF), pltpu.SemaphoreType.DMA((3,))],
        name="up_proj",
        **params(8_700_000_000, 28_000_000, 32),
    )(
        core_in,
        table,
        tokens,
        other,
        partial_attn,
        other_attn,
        post_gain,
        feedforward_pre_gain.reshape(1, -1),
        *up_w,
    )

    def down_half(side):
        return pl.pallas_call(
            down_kernel,
            grid=grid,
            in_specs=[SMEM, SMEM, rows_of(block, 2048)] + [HBM] * 6,
            out_specs=rows_of(block, 1024),
            out_shape=jax.ShapeDtypeStruct((length, 1024), BF),
            scratch_shapes=[pltpu.VMEM((1024, 2048), BF), pltpu.SemaphoreType.DMA((3,))],
            **params(4_300_000_000, 10_000_000, 16),
        )(table, side, squared, *down_w)

    away = down_half(1 - core_in)
    theirs = swap_cores(away)
    mine = down_half(core_in)
    feed = mine.astype(F32) + theirs.astype(F32)
    squares = jnp.sum(feed * feed, axis=1)
    squares_other = swap_cores(squares.reshape(8, 128)).reshape(length)
    scale = lax.rsqrt((squares + squares_other) / 2048 + EPS)[:, None]
    resid_own = lax.dynamic_slice_in_dim(resid, core * 1024, 1024, axis=1)
    return (resid_own.astype(F32) + feed * scale * feedforward_post_gain).astype(BF)


def solution(mesh):
    finer = Mesh(
        mesh.devices.reshape(mesh.shape["rep"], 2, 4, 4, mesh.shape["tp"]),
        ("rep", "fs_0", "fs_1", "fs_2", "tp"),
    )
    in_specs = (
        P(REP_FS, "tp"),
        P(),
        P(FS, "tp"),
        P(FS, "tp"),
        P(FS, "tp"),
        P(),
        P(None, "tp"),
        P("tp"),
        P(REP_FS, "tp"),
        P(),
        P("tp", FS),
        P("tp"),
        P(),
        P(FS, "tp"),
        P("tp", FS),
        P("tp"),
    )

    return jax.shard_map(
        on_device, mesh=finer, in_specs=in_specs, out_specs=P(REP_FS, "tp"), check_vma=False
    )
```

```python
import jax
import jax.numpy as jnp
import numpy as np
from jax import lax
from jax.experimental import pallas as pl
from jax.experimental.pallas import tpu as pltpu
from jax.sharding import Mesh
from jax.sharding import PartitionSpec as P


FS = ("fs_0", "fs_1", "fs_2")
REP_FS = ("rep", "fs_0", "fs_1", "fs_2")
ALL = ("rep", "fs_0", "fs_1", "fs_2", "tp")
EPS = 1e-06
CHUNK = 256
HALF = 32
BF = jnp.bfloat16
F32 = jnp.float32


CLASSES = (("x", 1), ("y", 1), ("z", 1), ("x", 3), ("y", 3), ("z", 3))


def link_class(step, chain, core):
    if step < 3:
        return CLASSES[3 * core + step]
    return CLASSES[3 * (1 - core) + (step + chain) % 3]


def partner_pairs(step, chain):
    pairs = []
    for z in range(4):
        for y in range(4):
            for x in range(4):
                for core in range(2):
                    axis, flip = link_class(step, chain, core)
                    to = {"x": x, "y": y, "z": z}
                    to[axis] ^= flip
                    source = ((z * 4 + y) * 4 + x) * 2 + core
                    target = ((to["z"] * 4 + to["y"]) * 4 + to["x"]) * 2 + core
                    pairs.append((source, target))
    return pairs


def row_block(z, y, x):
    return (((z & 1) * 16 + y * 4 + x) << 1) | (z >> 1)


def block_offsets():
    table = np.zeros((2, 6, 64), np.int32)
    for core in range(2):
        for row in range(6):
            for place in range(64):
                total = 0
                for step in range(6):
                    if place >> step & 1:
                        axis, flip = link_class(step, row % 3, core)
                        at = {"x": 0, "y": 0, "z": 0}
                        at[axis] = flip
                        total ^= row_block(at["z"], at["y"], at["x"])
                table[core, row, place] = total
    return table


OFFSETS = block_offsets()


def half_places():
    lists = np.zeros((2, 2, 6, 16), np.int32)
    for core in range(2):
        for high in range(2):
            for chain in range(3):
                for piece in range(2):
                    offsets = OFFSETS[core, 3 + chain, 32 * piece : 32 * piece + 32]
                    lists[core, high, 2 * chain + piece] = np.flatnonzero(offsets >> 5 == high)
    return lists


HALF_PLACES = half_places()


def half_targets():
    targets = np.zeros_like(HALF_PLACES)
    for core, high, row in np.ndindex(2, 2, 6):
        places = HALF_PLACES[core, high, row] + 32 * (row % 2)
        targets[core, high, row] = OFFSETS[core, 3 + row // 2, places] & 31
    return targets


HALF_TARGETS = half_targets()


def swap_cores(array):
    return lax.ppermute(array, "tp", [(0, 1), (1, 0)])


def over_link(array, step, chain):
    return lax.ppermute(array, ALL, partner_pairs(step, chain))


def joined(a, b):
    return jnp.concatenate([a, b], axis=0)


def gather_start(own):
    held = own
    for step in range(3):
        came = over_link(held, step, 0)
        if step < 2:
            held = joined(held, came)
    return held, came


def columns(pair, lane, width):
    return joined(*(a[:, lane : lane + width] for a in pair))


def block_copy(piece, at, target, to, lane, sem):
    pltpu.make_async_copy(
        piece.at[pl.ds(pl.multiple_of(at * HALF, HALF), HALF), :],
        target.at[pl.ds(pl.multiple_of(to * HALF, HALF), HALF), pl.ds(lane, piece.shape[1])],
        sem,
    ).start()


def place_blocks(table, row, pieces, target, lane, sem):
    place = 0
    for piece in pieces:
        count = piece.shape[0] // HALF

        def one(i, carry, piece=piece, place=place):
            block_copy(piece, i, target, table[row, place + i], lane, sem)
            return carry

        lax.fori_loop(0, count, one, 0, unroll=4)
        place += count


def place_half(places, targets, row, pieces, target, lane, sem):
    for k, piece in enumerate(pieces):

        def one(i, carry, piece=piece, k=k):
            block_copy(
                piece, places[2 * row + k, i], target, targets[2 * row + k, i], lane, sem
            )
            return carry

        lax.fori_loop(0, 16, one, 0, unroll=4)


def wait_part(target, lane, width, sem):
    part = target.at[:, pl.ds(lane, width)]
    pltpu.make_async_copy(part, part, sem).wait()


def nt_dot(a, b):
    return lax.dot_general(a, b, (((1,), (1,)), ((), ())), preferred_element_type=F32)


def tn_dot(a, b):
    return lax.dot_general(a, b, (((0,), (0,)), ((), ())), preferred_element_type=F32)


def ordered(core, own, other):
    first = core == 0
    return jnp.concatenate([jnp.where(first, own, other), jnp.where(first, other, own)], axis=1)


def norm_kernel(core, own, other, gain, first, second, bias, surge, normed_out, decay_out):
    rows = ordered(core[0], own[...], other[...]).astype(F32)
    scale = lax.rsqrt(jnp.mean(rows * rows, axis=-1, keepdims=True) + EPS)
    normed = (rows * scale * gain[...]).astype(BF)
    normed_out[...] = normed
    rank = jnp.dot(normed, first[...], preferred_element_type=F32).astype(BF)
    gate = jnp.dot(rank, second[...], preferred_element_type=F32) + bias[...]
    decay_out[...] = jax.nn.log_sigmoid(gate) / 16.0 + surge[...]


def small_level_matrices():
    i = np.arange(CHUNK)[:, None]
    t = np.arange(CHUNK)[None, :]
    mats = []
    for size in (2, 4):
        same = i // (2 * size) == t // (2 * size)
        upper_i, upper_t = i % (2 * size) >= size, t % (2 * size) >= size
        mats.append(same & ((upper_i & upper_t & (t <= i)) | (~upper_i & ~upper_t & (t > i))))
    same = i // 8 == t // 8
    mats.append(same & (t <= i))
    mats.append(same & (t > i))
    return np.concatenate(mats, axis=0)


def level_of_pairs():
    i = np.arange(CHUNK)[:, None]
    j = np.arange(CHUNK)[None, :]
    level = np.floor(np.log2(np.maximum(i ^ j, 1))).astype(np.int32)
    return np.where(j < i, level, -1).astype(np.int32)


SMALL_LEVELS = small_level_matrices()
PAIR_LEVELS = level_of_pairs()


def attention_kernel(table, normed, decay, mats, pair_level, gain, *rest):
    pieces = (rest[0:2], rest[2:4], rest[4:6])
    partial_out, w_qk, w_v, w_out, state, sems = rest[6:]
    weights = (w_qk, w_v, w_out)
    for c in range(3):
        place_blocks(table, c, pieces[c], weights[c], 0, sems.at[c])
    state[...] = jnp.zeros_like(state)
    for c in range(3):
        wait_part(weights[c], 0, 512, sems.at[c])

    def one(i, carry):
        here = pl.ds(pl.multiple_of(i * CHUNK, CHUNK), CHUNK)
        partial_out[here, :] = attention_chunk(
            normed[here, :], decay[here, :], mats, pair_level, gain, w_qk, w_v, w_out, state
        )
        return carry

    lax.fori_loop(0, normed.shape[0] // CHUNK, one, 0)


def attention_chunk(rows, g, mats, pair_level, gain, w_qk, w_v, w_out, state):
    g_hi = g.astype(BF)
    g_lo = (g - g_hi.astype(F32)).astype(BF)

    def summed(index):
        mat = mats[pl.ds(index * CHUNK, CHUNK), :]
        return jnp.dot(mat, g_hi, preferred_element_type=F32) + jnp.dot(
            mat, g_lo, preferred_element_type=F32
        )

    before, after = summed(2), summed(3)
    row = lax.broadcasted_iota(jnp.int32, (CHUNK, CHUNK), 0)
    spans = [jnp.where((row & 1) != 0, g, 0.0), summed(0), summed(1)]
    size = 8
    while size < CHUNK:
        b = before.reshape(CHUNK // (2 * size), 2, size, CHUNK)
        a = after.reshape(CHUNK // (2 * size), 2, size, CHUNK)
        spans.append(jnp.stack([a[:, 0], b[:, 1]], axis=1).reshape(CHUNK, CHUNK))
        low, high = b[:, 0, size - 1 :, :], b[:, 1, size - 1 :, :]
        before = jnp.stack([b[:, 0], b[:, 1] + low], axis=1).reshape(CHUNK, CHUNK)
        after = jnp.stack([a[:, 0] + high, a[:, 1]], axis=1).reshape(CHUNK, CHUNK)
        size *= 2

    qk = jnp.dot(rows, w_qk[...], preferred_element_type=F32).astype(BF).astype(F32)
    q, k = qk[:, :256] * (256**-0.5), qk[:, 256:]
    v = jnp.dot(rows, w_v[...], preferred_element_type=F32).astype(BF)
    level_map = pair_level[...]
    scores = jnp.zeros((CHUNK, CHUNK), F32)
    for level, span in enumerate(spans):
        both = (jnp.where((row & (1 << level)) != 0, q, k) * jnp.exp(span)).astype(BF)
        scores = jnp.where(level_map == level, nt_dot(both, both), scores)
    q_in = (q * jnp.exp(before)).astype(BF)
    k_out = (k * jnp.exp(after)).astype(BF)
    old = state[...]
    readout = (
        nt_dot(q_in, old.astype(BF))
        + jnp.dot(scores.astype(BF), v, preferred_element_type=F32)
        + jnp.sum(q * k, axis=1, keepdims=True) * v.astype(F32)
    )
    state[...] = old * jnp.exp(before[CHUNK - 1 :, :]) + tn_dot(v, k_out)
    scale = lax.rsqrt(jnp.mean(readout * readout, axis=-1, keepdims=True) + EPS)
    mixed = (readout * scale * gain[...]).astype(BF)
    return nt_dot(mixed, w_out[...]).astype(BF)


UP_WIDTHS = (768, 640, 640)
DOWN_WIDTHS = (640, 640, 768)


def start_of(widths, chain):
    return sum(widths[:chain])


def middle_kernel(core, own, other, mine, theirs, gain_own, gain_other, pre_gain, resid_out, out):
    first = core[0] == 0
    rows = ordered(core[0], own[...], other[...]).astype(F32)
    post_gain = ordered(core[0], gain_own[...], gain_other[...])
    attn = mine[...].astype(F32) + theirs[...].astype(F32)
    scale = lax.rsqrt(jnp.mean(attn * attn, axis=-1, keepdims=True) + EPS)
    resid = (rows + attn * scale * post_gain).astype(BF)
    resid_out[...] = jnp.where(first, resid[:, :1024], resid[:, 1024:])
    values = resid.astype(F32)
    scale = lax.rsqrt(jnp.mean(values * values, axis=-1, keepdims=True) + EPS)
    out[...] = (values * scale * pre_gain[...]).astype(BF)


def up_kernel(table, normed, *rest):
    squared_out, weight, sems = rest[6:]
    for c in range(3):
        at = start_of(UP_WIDTHS, c)
        place_blocks(table, 3 + c, rest[2 * c : 2 * c + 2], weight, at, sems.at[c])
    for c in range(3):
        at, width = start_of(UP_WIDTHS, c), UP_WIDTHS[c]
        wait_part(weight, at, width, sems.at[c])

        def one(i, carry, at=at, width=width):
            here = pl.ds(pl.multiple_of(i * 256, 256), 256)
            hidden = jnp.dot(
                normed[here, :], weight[:, at : at + width], preferred_element_type=F32
            )
            hidden = jnp.maximum(hidden, 0.0)
            squared_out[here, at : at + width] = (hidden * hidden).astype(BF)
            return carry

        lax.fori_loop(0, normed.shape[0] // 256, one, 0)


def down_kernel(places, targets, squared, *rest):
    partial_out, weight, sems = rest[6:]
    for c in range(3):
        at = start_of(DOWN_WIDTHS, c)
        place_half(places, targets, c, rest[2 * c : 2 * c + 2], weight, at, sems.at[c])
    for c in range(3):
        wait_part(weight, start_of(DOWN_WIDTHS, c), DOWN_WIDTHS[c], sems.at[c])

    def one(i, carry):
        here = pl.ds(pl.multiple_of(i * 256, 256), 256)
        partial_out[here, :] = nt_dot(squared[here, :], weight[...]).astype(BF)
        return carry

    lax.fori_loop(0, squared.shape[0] // 256, one, 0)


SMEM = pl.BlockSpec(memory_space=pltpu.SMEM)
VMEM = pl.BlockSpec(memory_space=pltpu.VMEM)
HBM = pl.BlockSpec(memory_space=pltpu.HBM)


def whole(shape):
    return pl.BlockSpec(shape, lambda i: (0,) * len(shape))


def rows_of(count, width):
    return pl.BlockSpec((count, width), lambda i: (i, 0))


def params(flops, nbytes, vmem_mib):
    return dict(
        compiler_params=pltpu.CompilerParams(vmem_limit_bytes=vmem_mib * 1024 * 1024),
        cost_estimate=pl.CostEstimate(flops=flops, bytes_accessed=nbytes, transcendentals=0),
    )


def on_device(
    tokens,
    attention_pre_gain,
    query_matrix,
    key_matrix,
    value_matrix,
    decay_first_weight,
    decay_second_weight,
    decay_offset_bias,
    extra_log_surge,
    readout_head_gain,
    output_matrix,
    attention_post_gain,
    feedforward_pre_gain,
    up_matrix,
    down_matrix,
    feedforward_post_gain,
):
    length = tokens.shape[0]
    rep, core = lax.axis_index("rep"), lax.axis_index("tp")
    fs = lax.axis_index(FS)
    mine_block = (fs * 2 + rep).astype(jnp.int32)
    core_in = core.astype(jnp.int32).reshape(1)
    table = jnp.asarray(OFFSETS)[core] ^ mine_block

    def half(shard):
        return lax.dynamic_slice_in_dim(shard, rep * HALF, HALF, axis=0)

    first = jnp.concatenate(
        [half(query_matrix), half(key_matrix), half(value_matrix), half(output_matrix.T)], axis=1
    )
    first = gather_start(first)
    up, down = half(up_matrix), half(down_matrix.T)
    feed = []
    for c in range(3):
        a, b = start_of(UP_WIDTHS, c), start_of(DOWN_WIDTHS, c)
        feed += [up[:, a : a + UP_WIDTHS[c]], down[:, b : b + DOWN_WIDTHS[c]]]
    feed = gather_start(jnp.concatenate(feed, axis=1))
    first_w, up_w, down_w = [], [], []
    lane = 0
    for c in range(3):
        held = columns(first, 512 * c, 512)
        for step in (3, 4):
            held = joined(held, over_link(held, step, c))
        first_w += [held, over_link(held, 5, c)]

        a, b = UP_WIDTHS[c], DOWN_WIDTHS[c]
        held = columns(feed, lane, a + b)
        lane += a + b
        held = joined(held, over_link(held, 3, c))
        pair = held, over_link(held, 4, c)
        held = columns(pair, 0, a)
        up_w += [held, over_link(held, 5, c)]
        held = columns(pair, a, b)
        down_w += [held, over_link(held, 5, c)]

    other = swap_cores(tokens)
    block = 256
    grid = (length // block,)
    normed, decay = pl.pallas_call(
        norm_kernel,
        grid=grid,
        in_specs=[
            SMEM,
            rows_of(block, 1024),
            rows_of(block, 1024),
            whole((1, 2048)),
            whole((2048, 16)),
            whole((16, 256)),
            whole((1, 256)),
            rows_of(block, 1),
        ],
        out_specs=[rows_of(block, 2048), rows_of(block, 256)],
        out_shape=[
            jax.ShapeDtypeStruct((length, 2048), BF),
            jax.ShapeDtypeStruct((length, 256), F32),
        ],
        name="norm",
        **params(400_000_000, 10_000_000, 16),
    )(
        core_in,
        tokens,
        other,
        attention_pre_gain.reshape(1, -1),
        decay_first_weight,
        decay_second_weight,
        decay_offset_bias.reshape(1, -1),
        extra_log_surge,
    )
    partial_attn = pl.pallas_call(
        attention_kernel,
        in_specs=[SMEM] + [VMEM] * 5 + [HBM] * 6,
        out_specs=VMEM,
        out_shape=jax.ShapeDtypeStruct((length, 2048), BF),
        scratch_shapes=[
            pltpu.VMEM((2048, 512), BF),
            pltpu.VMEM((2048, 512), BF),
            pltpu.VMEM((2048, 512), BF),
            pltpu.VMEM((512, 256), F32),
            pltpu.SemaphoreType.DMA((3,)),
        ],
        name="attention",
        **params(11_000_000_000, 14_000_000, 26),
    )(
        table,
        normed,
        decay,
        jnp.asarray(SMALL_LEVELS, BF),
        jnp.asarray(PAIR_LEVELS),
        readout_head_gain.reshape(1, -1),
        *first_w,
    )
    other_attn = swap_cores(partial_attn)
    other_gain = swap_cores(attention_post_gain)
    resid, normed_mid = pl.pallas_call(
        middle_kernel,
        grid=grid,
        in_specs=[
            SMEM,
            rows_of(block, 1024),
            rows_of(block, 1024),
            rows_of(block, 2048),
            rows_of(block, 2048),
            whole((1, 1024)),
            whole((1, 1024)),
            whole((1, 2048)),
        ],
        out_specs=[rows_of(block, 1024), rows_of(block, 2048)],
        out_shape=[
            jax.ShapeDtypeStruct((length, 1024), BF),
            jax.ShapeDtypeStruct((length, 2048), BF),
        ],
        name="middle",
        **params(60_000_000, 18_000_000, 20),
    )(
        core_in,
        tokens,
        other,
        partial_attn,
        other_attn,
        attention_post_gain.reshape(1, -1),
        other_gain.reshape(1, -1),
        feedforward_pre_gain.reshape(1, -1),
    )
    squared = pl.pallas_call(
        up_kernel,
        in_specs=[SMEM, VMEM] + [HBM] * 6,
        out_specs=VMEM,
        out_shape=jax.ShapeDtypeStruct((length, 2048), BF),
        scratch_shapes=[pltpu.VMEM((2048, 2048), BF), pltpu.SemaphoreType.DMA((3,))],
        name="up_proj",
        **params(8_700_000_000, 16_000_000, 24),
    )(table, normed_mid, *up_w)

    def down_half(side):
        return pl.pallas_call(
            down_kernel,
            in_specs=[SMEM, SMEM, VMEM] + [HBM] * 6,
            out_specs=VMEM,
            out_shape=jax.ShapeDtypeStruct((length, 1024), BF),
            scratch_shapes=[pltpu.VMEM((1024, 2048), BF), pltpu.SemaphoreType.DMA((3,))],
            **params(4_300_000_000, 10_000_000, 20),
        )(
            jnp.asarray(HALF_PLACES)[core, side ^ (mine_block >> 5)],
            jnp.asarray(HALF_TARGETS)[core, side ^ (mine_block >> 5)] ^ (mine_block & 31),
            squared,
            *down_w,
        )

    away = down_half(1 - core)
    theirs = swap_cores(away)
    mine = down_half(core)
    feed = mine.astype(F32) + theirs.astype(F32)
    squares = jnp.sum(feed * feed, axis=1)
    squares_other = swap_cores(squares.reshape(8, 128)).reshape(length)
    scale = lax.rsqrt((squares + squares_other) / 2048 + EPS)[:, None]
    return (resid.astype(F32) + feed * scale * feedforward_post_gain).astype(BF)


def solution(mesh):
    finer = Mesh(
        mesh.devices.reshape(mesh.shape["rep"], 2, 4, 4, mesh.shape["tp"]),
        ("rep", "fs_0", "fs_1", "fs_2", "tp"),
    )
    in_specs = (
        P(REP_FS, "tp"),
        P(),
        P(FS, "tp"),
        P(FS, "tp"),
        P(FS, "tp"),
        P(),
        P(None, "tp"),
        P("tp"),
        P(REP_FS, "tp"),
        P(),
        P("tp", FS),
        P("tp"),
        P(),
        P(FS, "tp"),
        P("tp", FS),
        P("tp"),
    )

    return jax.shard_map(
        on_device, mesh=finer, in_specs=in_specs, out_specs=P(REP_FS, "tp"), check_vma=False
    )
```

```python
import jax
import jax.numpy as jnp
import numpy as np
from jax import lax
from jax.experimental import pallas as pl
from jax.experimental.pallas import tpu as pltpu
from jax.sharding import Mesh
from jax.sharding import PartitionSpec as P


FS = ("fs_0", "fs_1", "fs_2")
REP_FS = ("rep", "fs_0", "fs_1", "fs_2")
ALL = ("rep", "fs_0", "fs_1", "fs_2", "tp")
EPS = 1e-06
CHUNK = 256
HALF = 32
BF = jnp.bfloat16
F32 = jnp.float32


CLASSES = (("x", 1), ("y", 1), ("z", 1), ("x", 3), ("y", 3), ("z", 3))


def link_class(step, chain, core):
    if step < 3:
        return CLASSES[3 * core + step]
    return CLASSES[3 * (1 - core) + (step + chain) % 3]


def partner_pairs(step, chain):
    pairs = []
    for z in range(4):
        for y in range(4):
            for x in range(4):
                for core in range(2):
                    axis, flip = link_class(step, chain, core)
                    to = {"x": x, "y": y, "z": z}
                    to[axis] ^= flip
                    source = ((z * 4 + y) * 4 + x) * 2 + core
                    target = ((to["z"] * 4 + to["y"]) * 4 + to["x"]) * 2 + core
                    pairs.append((source, target))
    return pairs


def row_block(z, y, x):
    return (((z & 1) * 16 + y * 4 + x) << 1) | (z >> 1)


def block_offsets():
    table = np.zeros((2, 6, 64), np.int32)
    for core in range(2):
        for row in range(6):
            for place in range(64):
                total = 0
                for step in range(6):
                    if place >> step & 1:
                        axis, flip = link_class(step, row % 3, core)
                        at = {"x": 0, "y": 0, "z": 0}
                        at[axis] = flip
                        total ^= row_block(at["z"], at["y"], at["x"])
                table[core, row, place] = total
    return table


OFFSETS = block_offsets()


def half_places():
    lists = np.zeros((2, 2, 6, 16), np.int32)
    for core in range(2):
        for high in range(2):
            for chain in range(3):
                for piece in range(2):
                    offsets = OFFSETS[core, 3 + chain, 32 * piece : 32 * piece + 32]
                    lists[core, high, 2 * chain + piece] = np.flatnonzero(offsets >> 5 == high)
    return lists


HALF_PLACES = half_places()


def half_targets():
    targets = np.zeros_like(HALF_PLACES)
    for core, high, row in np.ndindex(2, 2, 6):
        places = HALF_PLACES[core, high, row] + 32 * (row % 2)
        targets[core, high, row] = OFFSETS[core, 3 + row // 2, places] & 31
    return targets


HALF_TARGETS = half_targets()


def swap_cores(array):
    return lax.ppermute(array, "tp", [(0, 1), (1, 0)])


def over_link(array, step, chain):
    return lax.ppermute(array, ALL, partner_pairs(step, chain))


def joined(a, b):
    return jnp.concatenate([a, b], axis=0)


def gather_start(own):
    held = own
    for step in range(3):
        came = over_link(held, step, 0)
        if step < 2:
            held = joined(held, came)
    return held, came


def columns(pair, lane, width):
    return joined(*(a[:, lane : lane + width] for a in pair))


def block_copy(piece, at, target, to, lane, sem):
    pltpu.make_async_copy(
        piece.at[pl.ds(pl.multiple_of(at * HALF, HALF), HALF), :],
        target.at[pl.ds(pl.multiple_of(to * HALF, HALF), HALF), pl.ds(lane, piece.shape[1])],
        sem,
    ).start()


def place_blocks(table, row, pieces, target, lane, sem):
    place = 0
    for piece in pieces:
        count = piece.shape[0] // HALF

        def one(i, carry, piece=piece, place=place):
            block_copy(piece, i, target, table[row, place + i], lane, sem)
            return carry

        lax.fori_loop(0, count, one, 0, unroll=4)
        place += count


def place_half(places, targets, row, pieces, target, lane, sem):
    for k, piece in enumerate(pieces):

        def one(i, carry, piece=piece, k=k):
            block_copy(
                piece, places[2 * row + k, i], target, targets[2 * row + k, i], lane, sem
            )
            return carry

        lax.fori_loop(0, 16, one, 0, unroll=4)


def wait_part(target, lane, width, sem):
    part = target.at[:, pl.ds(lane, width)]
    pltpu.make_async_copy(part, part, sem).wait()


def nt_dot(a, b):
    return lax.dot_general(a, b, (((1,), (1,)), ((), ())), preferred_element_type=F32)


def tn_dot(a, b):
    return lax.dot_general(a, b, (((0,), (0,)), ((), ())), preferred_element_type=F32)


def ordered(core, own, other):
    first = core == 0
    return jnp.concatenate([jnp.where(first, own, other), jnp.where(first, other, own)], axis=1)


def norm_kernel(core, own, other, gain, first, second, bias, surge, normed_out, decay_out):
    rows = ordered(core[0], own[...], other[...]).astype(F32)
    scale = lax.rsqrt(jnp.mean(rows * rows, axis=-1, keepdims=True) + EPS)
    normed = (rows * scale * gain[...]).astype(BF)
    normed_out[...] = normed
    rank = jnp.dot(normed, first[...], preferred_element_type=F32).astype(BF)
    gate = jnp.dot(rank, second[...], preferred_element_type=F32) + bias[...]
    decay_out[...] = jax.nn.log_sigmoid(gate) / 16.0 + surge[...]


def small_level_matrices():
    i = np.arange(CHUNK)[:, None]
    t = np.arange(CHUNK)[None, :]
    mats = []
    for size in (2, 4):
        same = i // (2 * size) == t // (2 * size)
        upper_i, upper_t = i % (2 * size) >= size, t % (2 * size) >= size
        mats.append(same & ((upper_i & upper_t & (t <= i)) | (~upper_i & ~upper_t & (t > i))))
    same = i // 8 == t // 8
    mats.append(same & (t <= i))
    mats.append(same & (t > i))
    return np.concatenate(mats, axis=0)


def level_of_pairs():
    i = np.arange(CHUNK)[:, None]
    j = np.arange(CHUNK)[None, :]
    level = np.floor(np.log2(np.maximum(i ^ j, 1))).astype(np.int32)
    return np.where(j < i, level, -1).astype(np.int32)


SMALL_LEVELS = small_level_matrices()
PAIR_LEVELS = level_of_pairs()


def attention_kernel(table, normed, decay, mats, pair_level, gain, *rest):
    pieces = (rest[0:2], rest[2:4], rest[4:6])
    partial_out, w_qk, w_v, w_out, state, sems = rest[6:]
    weights = (w_qk, w_v, w_out)
    for c in range(3):
        place_blocks(table, c, pieces[c], weights[c], 0, sems.at[c])
    state[...] = jnp.zeros_like(state)
    for c in range(3):
        wait_part(weights[c], 0, 512, sems.at[c])

    def one(i, carry):
        here = pl.ds(pl.multiple_of(i * CHUNK, CHUNK), CHUNK)
        partial_out[here, :] = attention_chunk(
            normed[here, :], decay[here, :], mats, pair_level, gain, w_qk, w_v, w_out, state
        )
        return carry

    lax.fori_loop(0, normed.shape[0] // CHUNK, one, 0)


def attention_chunk(rows, g, mats, pair_level, gain, w_qk, w_v, w_out, state):
    g_hi = g.astype(BF)
    g_lo = (g - g_hi.astype(F32)).astype(BF)

    def summed(index):
        mat = mats[pl.ds(index * CHUNK, CHUNK), :]
        return jnp.dot(mat, g_hi, preferred_element_type=F32) + jnp.dot(
            mat, g_lo, preferred_element_type=F32
        )

    before, after = summed(2), summed(3)
    row = lax.broadcasted_iota(jnp.int32, (CHUNK, CHUNK), 0)
    spans = [jnp.where((row & 1) != 0, g, 0.0), summed(0), summed(1)]
    size = 8
    while size < CHUNK:
        b = before.reshape(CHUNK // (2 * size), 2, size, CHUNK)
        a = after.reshape(CHUNK // (2 * size), 2, size, CHUNK)
        spans.append(jnp.stack([a[:, 0], b[:, 1]], axis=1).reshape(CHUNK, CHUNK))
        low, high = b[:, 0, size - 1 :, :], b[:, 1, size - 1 :, :]
        before = jnp.stack([b[:, 0], b[:, 1] + low], axis=1).reshape(CHUNK, CHUNK)
        after = jnp.stack([a[:, 0] + high, a[:, 1]], axis=1).reshape(CHUNK, CHUNK)
        size *= 2

    qk = jnp.dot(rows, w_qk[...], preferred_element_type=F32).astype(BF).astype(F32)
    q, k = qk[:, :256] * (256**-0.5), qk[:, 256:]
    v = jnp.dot(rows, w_v[...], preferred_element_type=F32).astype(BF)
    level_map = pair_level[...]
    scores = jnp.zeros((CHUNK, CHUNK), F32)
    for level, span in enumerate(spans):
        both = (jnp.where((row & (1 << level)) != 0, q, k) * jnp.exp(span)).astype(BF)
        scores = jnp.where(level_map == level, nt_dot(both, both), scores)
    q_in = (q * jnp.exp(before)).astype(BF)
    k_out = (k * jnp.exp(after)).astype(BF)
    old = state[...]
    readout = (
        nt_dot(q_in, old.astype(BF))
        + jnp.dot(scores.astype(BF), v, preferred_element_type=F32)
        + jnp.sum(q * k, axis=1, keepdims=True) * v.astype(F32)
    )
    state[...] = old * jnp.exp(before[CHUNK - 1 :, :]) + tn_dot(v, k_out)
    scale = lax.rsqrt(jnp.mean(readout * readout, axis=-1, keepdims=True) + EPS)
    mixed = (readout * scale * gain[...]).astype(BF)
    return nt_dot(mixed, w_out[...]).astype(BF)


UP_WIDTHS = (768, 640, 640)
DOWN_WIDTHS = (640, 768, 640)


def start_of(widths, chain):
    return sum(widths[:chain])


def middle_kernel(core, own, other, mine, theirs, gain_own, gain_other, pre_gain, resid_out, out):
    first = core[0] == 0
    rows = ordered(core[0], own[...], other[...]).astype(F32)
    post_gain = ordered(core[0], gain_own[...], gain_other[...])
    attn = mine[...].astype(F32) + theirs[...].astype(F32)
    scale = lax.rsqrt(jnp.mean(attn * attn, axis=-1, keepdims=True) + EPS)
    resid = (rows + attn * scale * post_gain).astype(BF)
    resid_out[...] = jnp.where(first, resid[:, :1024], resid[:, 1024:])
    values = resid.astype(F32)
    scale = lax.rsqrt(jnp.mean(values * values, axis=-1, keepdims=True) + EPS)
    out[...] = (values * scale * pre_gain[...]).astype(BF)


def up_kernel(table, normed_hbm, *rest):
    squared_out, weight, normed, sems = rest[6:]
    fetch = pltpu.make_async_copy(normed_hbm, normed, sems.at[3])
    fetch.start()
    for c in range(3):
        at = start_of(UP_WIDTHS, c)
        place_blocks(table, 3 + c, rest[2 * c : 2 * c + 2], weight, at, sems.at[c])
    for c in range(3):
        wait_part(weight, start_of(UP_WIDTHS, c), UP_WIDTHS[c], sems.at[c])
    fetch.wait()

    def one(i, carry):
        here = pl.ds(pl.multiple_of(i * 256, 256), 256)
        hidden = jnp.dot(normed[here, :], weight[...], preferred_element_type=F32)
        hidden = jnp.maximum(hidden, 0.0)
        squared_out[here, :] = (hidden * hidden).astype(BF)
        return carry

    lax.fori_loop(0, normed.shape[0] // 256, one, 0)


def down_kernel(places, targets, squared, *rest):
    partial_out, weight, sems = rest[6:]
    for c in range(3):
        at = start_of(DOWN_WIDTHS, c)
        place_half(places, targets, c, rest[2 * c : 2 * c + 2], weight, at, sems.at[c])
    for c in range(3):
        wait_part(weight, start_of(DOWN_WIDTHS, c), DOWN_WIDTHS[c], sems.at[c])

    def one(i, carry):
        here = pl.ds(pl.multiple_of(i * 256, 256), 256)
        partial_out[here, :] = nt_dot(squared[here, :], weight[...]).astype(BF)
        return carry

    lax.fori_loop(0, squared.shape[0] // 256, one, 0)


SMEM = pl.BlockSpec(memory_space=pltpu.SMEM)
VMEM = pl.BlockSpec(memory_space=pltpu.VMEM)
HBM = pl.BlockSpec(memory_space=pltpu.HBM)


def whole(shape):
    return pl.BlockSpec(shape, lambda i: (0,) * len(shape))


def rows_of(count, width):
    return pl.BlockSpec((count, width), lambda i: (i, 0))


def params(flops, nbytes, vmem_mib):
    return dict(
        compiler_params=pltpu.CompilerParams(vmem_limit_bytes=vmem_mib * 1024 * 1024),
        cost_estimate=pl.CostEstimate(flops=flops, bytes_accessed=nbytes, transcendentals=0),
    )


def on_device(
    tokens,
    attention_pre_gain,
    query_matrix,
    key_matrix,
    value_matrix,
    decay_first_weight,
    decay_second_weight,
    decay_offset_bias,
    extra_log_surge,
    readout_head_gain,
    output_matrix,
    attention_post_gain,
    feedforward_pre_gain,
    up_matrix,
    down_matrix,
    feedforward_post_gain,
):
    length = tokens.shape[0]
    rep, core = lax.axis_index("rep"), lax.axis_index("tp")
    fs = lax.axis_index(FS)
    mine_block = (fs * 2 + rep).astype(jnp.int32)
    core_in = core.astype(jnp.int32).reshape(1)
    table = jnp.asarray(OFFSETS)[core] ^ mine_block

    def half(shard):
        return lax.dynamic_slice_in_dim(shard, rep * HALF, HALF, axis=0)

    first = jnp.concatenate(
        [half(query_matrix), half(key_matrix), half(value_matrix), half(output_matrix.T)], axis=1
    )
    first = gather_start(first)
    up, down = half(up_matrix), half(down_matrix.T)
    feed = []
    for c in range(3):
        a, b = start_of(UP_WIDTHS, c), start_of(DOWN_WIDTHS, c)
        feed += [up[:, a : a + UP_WIDTHS[c]], down[:, b : b + DOWN_WIDTHS[c]]]
    feed = gather_start(jnp.concatenate(feed, axis=1))
    first_w, up_w, down_w = [], [], []
    lane = 0
    for c in range(3):
        held = columns(first, 512 * c, 512)
        for step in (3, 4):
            held = joined(held, over_link(held, step, c))
        first_w += [held, over_link(held, 5, c)]

        a, b = UP_WIDTHS[c], DOWN_WIDTHS[c]
        held = columns(feed, lane, a + b)
        lane += a + b
        held = joined(held, over_link(held, 3, c))
        pair = held, over_link(held, 4, c)
        held = columns(pair, 0, a)
        up_w += [held, over_link(held, 5, c)]
        held = columns(pair, a, b)
        down_w += [held, over_link(held, 5, c)]

    other = swap_cores(tokens)
    block = 256
    grid = (length // block,)
    normed, decay = pl.pallas_call(
        norm_kernel,
        grid=grid,
        in_specs=[
            SMEM,
            rows_of(block, 1024),
            rows_of(block, 1024),
            whole((1, 2048)),
            whole((2048, 16)),
            whole((16, 256)),
            whole((1, 256)),
            rows_of(block, 1),
        ],
        out_specs=[rows_of(block, 2048), rows_of(block, 256)],
        out_shape=[
            jax.ShapeDtypeStruct((length, 2048), BF),
            jax.ShapeDtypeStruct((length, 256), F32),
        ],
        name="norm",
        **params(400_000_000, 10_000_000, 16),
    )(
        core_in,
        tokens,
        other,
        attention_pre_gain.reshape(1, -1),
        decay_first_weight,
        decay_second_weight,
        decay_offset_bias.reshape(1, -1),
        extra_log_surge,
    )
    partial_attn = pl.pallas_call(
        attention_kernel,
        in_specs=[SMEM] + [VMEM] * 5 + [HBM] * 6,
        out_specs=VMEM,
        out_shape=jax.ShapeDtypeStruct((length, 2048), BF),
        scratch_shapes=[
            pltpu.VMEM((2048, 512), BF),
            pltpu.VMEM((2048, 512), BF),
            pltpu.VMEM((2048, 512), BF),
            pltpu.VMEM((512, 256), F32),
            pltpu.SemaphoreType.DMA((3,)),
        ],
        name="attention",
        **params(11_000_000_000, 14_000_000, 26),
    )(
        table,
        normed,
        decay,
        jnp.asarray(SMALL_LEVELS, BF),
        jnp.asarray(PAIR_LEVELS),
        readout_head_gain.reshape(1, -1),
        *first_w,
    )
    other_attn = swap_cores(partial_attn)
    other_gain = swap_cores(attention_post_gain)
    resid, normed_mid = pl.pallas_call(
        middle_kernel,
        grid=grid,
        in_specs=[
            SMEM,
            rows_of(block, 1024),
            rows_of(block, 1024),
            rows_of(block, 2048),
            rows_of(block, 2048),
            whole((1, 1024)),
            whole((1, 1024)),
            whole((1, 2048)),
        ],
        out_specs=[rows_of(block, 1024), rows_of(block, 2048)],
        out_shape=[
            jax.ShapeDtypeStruct((length, 1024), BF),
            pltpu.HBM((length, 2048), BF),
        ],
        name="middle",
        **params(60_000_000, 18_000_000, 20),
    )(
        core_in,
        tokens,
        other,
        partial_attn,
        other_attn,
        attention_post_gain.reshape(1, -1),
        other_gain.reshape(1, -1),
        feedforward_pre_gain.reshape(1, -1),
    )
    normed_mid = pltpu.with_memory_space_constraint(normed_mid, pltpu.HBM)
    squared = pl.pallas_call(
        up_kernel,
        in_specs=[SMEM] + [HBM] * 7,
        out_specs=VMEM,
        out_shape=jax.ShapeDtypeStruct((length, 2048), BF),
        scratch_shapes=[
            pltpu.VMEM((2048, 2048), BF),
            pltpu.VMEM((length, 2048), BF),
            pltpu.SemaphoreType.DMA((4,)),
        ],
        name="up_proj",
        **params(8_700_000_000, 16_000_000, 24),
    )(table, normed_mid, *up_w)

    def down_half(side):
        return pl.pallas_call(
            down_kernel,
            in_specs=[SMEM, SMEM, VMEM] + [HBM] * 6,
            out_specs=VMEM,
            out_shape=jax.ShapeDtypeStruct((length, 1024), BF),
            scratch_shapes=[pltpu.VMEM((1024, 2048), BF), pltpu.SemaphoreType.DMA((3,))],
            **params(4_300_000_000, 10_000_000, 20),
        )(
            jnp.asarray(HALF_PLACES)[core, side ^ (mine_block >> 5)],
            jnp.asarray(HALF_TARGETS)[core, side ^ (mine_block >> 5)] ^ (mine_block & 31),
            squared,
            *down_w,
        )

    away = down_half(1 - core)
    theirs = swap_cores(away)
    mine = down_half(core)
    feed = mine.astype(F32) + theirs.astype(F32)
    squares = jnp.sum(feed * feed, axis=1)
    squares_other = swap_cores(squares.reshape(8, 128)).reshape(length)
    scale = lax.rsqrt((squares + squares_other) / 2048 + EPS)[:, None]
    return (resid.astype(F32) + feed * scale * feedforward_post_gain).astype(BF)


def solution(mesh):
    finer = Mesh(
        mesh.devices.reshape(mesh.shape["rep"], 2, 4, 4, mesh.shape["tp"]),
        ("rep", "fs_0", "fs_1", "fs_2", "tp"),
    )
    in_specs = (
        P(REP_FS, "tp"),
        P(),
        P(FS, "tp"),
        P(FS, "tp"),
        P(FS, "tp"),
        P(),
        P(None, "tp"),
        P("tp"),
        P(REP_FS, "tp"),
        P(),
        P("tp", FS),
        P("tp"),
        P(),
        P(FS, "tp"),
        P("tp", FS),
        P("tp"),
    )

    return jax.shard_map(
        on_device, mesh=finer, in_specs=in_specs, out_specs=P(REP_FS, "tp"), check_vma=False
    )
```

```python
import jax
import jax.numpy as jnp
import numpy as np
from jax import lax
from jax.experimental import pallas as pl
from jax.experimental.pallas import tpu as pltpu
from jax.sharding import Mesh
from jax.sharding import PartitionSpec as P


FS = ("fs_0", "fs_1", "fs_2")
REP_FS = ("rep", "fs_0", "fs_1", "fs_2")
ALL = ("rep", "fs_0", "fs_1", "fs_2", "tp")
EPS = 1e-06
CHUNK = 256
HALF = 32
BF = jnp.bfloat16
F32 = jnp.float32


CLASSES = (("x", 1), ("y", 1), ("z", 1), ("x", 3), ("y", 3), ("z", 3))


def link_class(step, chain, core):
    if step < 3:
        return CLASSES[3 * core + step]
    return CLASSES[3 * (1 - core) + (step + chain) % 3]


def partner_pairs(step, chain):
    pairs = []
    for z in range(4):
        for y in range(4):
            for x in range(4):
                for core in range(2):
                    axis, flip = link_class(step, chain, core)
                    to = {"x": x, "y": y, "z": z}
                    to[axis] ^= flip
                    source = ((z * 4 + y) * 4 + x) * 2 + core
                    target = ((to["z"] * 4 + to["y"]) * 4 + to["x"]) * 2 + core
                    pairs.append((source, target))
    return pairs


def row_block(z, y, x):
    return (((z & 1) * 16 + y * 4 + x) << 1) | (z >> 1)


def block_offsets():
    table = np.zeros((2, 6, 64), np.int32)
    for core in range(2):
        for row in range(6):
            for place in range(64):
                total = 0
                for step in range(6):
                    if place >> step & 1:
                        axis, flip = link_class(step, row % 3, core)
                        at = {"x": 0, "y": 0, "z": 0}
                        at[axis] = flip
                        total ^= row_block(at["z"], at["y"], at["x"])
                table[core, row, place] = total
    return table


OFFSETS = block_offsets()


def half_places():
    lists = np.zeros((2, 2, 6, 16), np.int32)
    for core in range(2):
        for high in range(2):
            for chain in range(3):
                for piece in range(2):
                    offsets = OFFSETS[core, 3 + chain, 32 * piece : 32 * piece + 32]
                    lists[core, high, 2 * chain + piece] = np.flatnonzero(offsets >> 5 == high)
    return lists


HALF_PLACES = half_places()


def half_targets():
    targets = np.zeros_like(HALF_PLACES)
    for core, high, row in np.ndindex(2, 2, 6):
        places = HALF_PLACES[core, high, row] + 32 * (row % 2)
        targets[core, high, row] = OFFSETS[core, 3 + row // 2, places] & 31
    return targets


HALF_TARGETS = half_targets()


def swap_cores(array):
    return lax.ppermute(array, "tp", [(0, 1), (1, 0)])


def over_link(array, step, chain):
    return lax.ppermute(array, ALL, partner_pairs(step, chain))


def joined(a, b):
    return jnp.concatenate([a, b], axis=0)


def gather_start(own):
    held = own
    for step in range(3):
        came = over_link(held, step, 0)
        if step < 2:
            held = joined(held, came)
    return held, came


def columns(pair, lane, width):
    return joined(*(a[:, lane : lane + width] for a in pair))


def block_copy(piece, at, target, to, lane, sem):
    pltpu.make_async_copy(
        piece.at[pl.ds(pl.multiple_of(at * HALF, HALF), HALF), :],
        target.at[pl.ds(pl.multiple_of(to * HALF, HALF), HALF), pl.ds(lane, piece.shape[1])],
        sem,
    ).start()


def place_blocks(table, row, pieces, target, lane, sem):
    place = 0
    for piece in pieces:
        count = piece.shape[0] // HALF

        def one(i, carry, piece=piece, place=place):
            block_copy(piece, i, target, table[row, place + i], lane, sem)
            return carry

        lax.fori_loop(0, count, one, 0, unroll=4)
        place += count


def place_half(places, targets, row, pieces, target, lane, sem):
    for k, piece in enumerate(pieces):

        def one(i, carry, piece=piece, k=k):
            block_copy(
                piece, places[2 * row + k, i], target, targets[2 * row + k, i], lane, sem
            )
            return carry

        lax.fori_loop(0, 16, one, 0, unroll=4)


def wait_part(target, lane, width, sem):
    part = target.at[:, pl.ds(lane, width)]
    pltpu.make_async_copy(part, part, sem).wait()


def nt_dot(a, b):
    return lax.dot_general(a, b, (((1,), (1,)), ((), ())), preferred_element_type=F32)


def tn_dot(a, b):
    return lax.dot_general(a, b, (((0,), (0,)), ((), ())), preferred_element_type=F32)


def ordered(core, own, other):
    first = core == 0
    return jnp.concatenate([jnp.where(first, own, other), jnp.where(first, other, own)], axis=1)


def norm_kernel(core, own, other, gain, first, second, bias, surge, normed_out, decay_out):
    rows = ordered(core[0], own[...], other[...]).astype(F32)
    scale = lax.rsqrt(jnp.mean(rows * rows, axis=-1, keepdims=True) + EPS)
    normed = (rows * scale * gain[...]).astype(BF)
    normed_out[...] = normed
    rank = jnp.dot(normed, first[...], preferred_element_type=F32).astype(BF)
    gate = jnp.dot(rank, second[...], preferred_element_type=F32) + bias[...]
    decay_out[...] = jax.nn.log_sigmoid(gate) / 16.0 + surge[...]


def small_level_matrices():
    i = np.arange(CHUNK)[:, None]
    t = np.arange(CHUNK)[None, :]
    mats = []
    for size in (2, 4):
        same = i // (2 * size) == t // (2 * size)
        upper_i, upper_t = i % (2 * size) >= size, t % (2 * size) >= size
        mats.append(same & ((upper_i & upper_t & (t <= i)) | (~upper_i & ~upper_t & (t > i))))
    same = i // 8 == t // 8
    mats.append(same & (t <= i))
    mats.append(same & (t > i))
    return np.concatenate(mats, axis=0)


def level_of_pairs():
    i = np.arange(CHUNK)[:, None]
    j = np.arange(CHUNK)[None, :]
    level = np.floor(np.log2(np.maximum(i ^ j, 1))).astype(np.int32)
    return np.where(j < i, level, -1).astype(np.int32)


SMALL_LEVELS = small_level_matrices()
PAIR_LEVELS = level_of_pairs()


def attention_kernel(table, normed, decay, mats, pair_level, gain, *rest):
    pieces = (rest[0:2], rest[2:4], rest[4:6])
    partial_out, w_qk, w_v, w_out, state, sems = rest[6:]
    weights = (w_qk, w_v, w_out)
    for c in range(3):
        place_blocks(table, c, pieces[c], weights[c], 0, sems.at[c])
    state[...] = jnp.zeros_like(state)
    for c in range(2):
        wait_part(weights[c], 0, 512, sems.at[c])

    def one(i, carry):
        here = pl.ds(pl.multiple_of(i * CHUNK, CHUNK), CHUNK)
        mixed = attention_chunk(
            normed[here, :], decay[here, :], mats, pair_level, gain, w_qk, w_v, state
        )

        @pl.when(i == 0)
        def _():
            wait_part(w_out, 0, 512, sems.at[2])

        partial_out[here, :] = nt_dot(mixed, w_out[...]).astype(BF)
        return carry

    lax.fori_loop(0, normed.shape[0] // CHUNK, one, 0)


def attention_chunk(rows, g, mats, pair_level, gain, w_qk, w_v, state):
    g_hi = g.astype(BF)
    g_lo = (g - g_hi.astype(F32)).astype(BF)

    def summed(index):
        mat = mats[pl.ds(index * CHUNK, CHUNK), :]
        return jnp.dot(mat, g_hi, preferred_element_type=F32) + jnp.dot(
            mat, g_lo, preferred_element_type=F32
        )

    before, after = summed(2), summed(3)
    row = lax.broadcasted_iota(jnp.int32, (CHUNK, CHUNK), 0)
    spans = [jnp.where((row & 1) != 0, g, 0.0), summed(0), summed(1)]
    size = 8
    while size < CHUNK:
        b = before.reshape(CHUNK // (2 * size), 2, size, CHUNK)
        a = after.reshape(CHUNK // (2 * size), 2, size, CHUNK)
        spans.append(jnp.stack([a[:, 0], b[:, 1]], axis=1).reshape(CHUNK, CHUNK))
        low, high = b[:, 0, size - 1 :, :], b[:, 1, size - 1 :, :]
        before = jnp.stack([b[:, 0], b[:, 1] + low], axis=1).reshape(CHUNK, CHUNK)
        after = jnp.stack([a[:, 0] + high, a[:, 1]], axis=1).reshape(CHUNK, CHUNK)
        size *= 2

    qk = jnp.dot(rows, w_qk[...], preferred_element_type=F32).astype(BF).astype(F32)
    q, k = qk[:, :256] * (256**-0.5), qk[:, 256:]
    v = jnp.dot(rows, w_v[...], preferred_element_type=F32).astype(BF)
    level_map = pair_level[...]
    scores = jnp.zeros((CHUNK, CHUNK), F32)
    for level, span in enumerate(spans):
        both = (jnp.where((row & (1 << level)) != 0, q, k) * jnp.exp(span)).astype(BF)
        scores = jnp.where(level_map == level, nt_dot(both, both), scores)
    q_in = (q * jnp.exp(before)).astype(BF)
    k_out = (k * jnp.exp(after)).astype(BF)
    old = state[...]
    readout = (
        nt_dot(q_in, old.astype(BF))
        + jnp.dot(scores.astype(BF), v, preferred_element_type=F32)
        + jnp.sum(q * k, axis=1, keepdims=True) * v.astype(F32)
    )
    state[...] = old * jnp.exp(before[CHUNK - 1 :, :]) + tn_dot(v, k_out)
    scale = lax.rsqrt(jnp.mean(readout * readout, axis=-1, keepdims=True) + EPS)
    return (readout * scale * gain[...]).astype(BF)


UP_WIDTHS = (768, 640, 640)
DOWN_WIDTHS = (640, 768, 640)


def start_of(widths, chain):
    return sum(widths[:chain])


def middle_kernel(core, own, other, mine, theirs, gain_own, gain_other, pre_gain, resid_out, out):
    first = core[0] == 0
    rows = ordered(core[0], own[...], other[...]).astype(F32)
    post_gain = ordered(core[0], gain_own[...], gain_other[...])
    attn = mine[...].astype(F32) + theirs[...].astype(F32)
    scale = lax.rsqrt(jnp.mean(attn * attn, axis=-1, keepdims=True) + EPS)
    resid = (rows + attn * scale * post_gain).astype(BF)
    resid_out[...] = jnp.where(first, resid[:, :1024], resid[:, 1024:])
    values = resid.astype(F32)
    scale = lax.rsqrt(jnp.mean(values * values, axis=-1, keepdims=True) + EPS)
    out[...] = (values * scale * pre_gain[...]).astype(BF)


def up_kernel(table, normed_hbm, *rest):
    squared_out, weight, normed, sems = rest[6:]

    def fetch(i):
        here = pl.ds(pl.multiple_of(i * 256, 256), 256)
        return pltpu.make_async_copy(normed_hbm.at[here, :], normed.at[here, :], sems.at[3 + i])

    fetch(0).start()
    for c in range(3):
        at = start_of(UP_WIDTHS, c)
        place_blocks(table, 3 + c, rest[2 * c : 2 * c + 2], weight, at, sems.at[c])
    for i in range(1, 4):
        fetch(i).start()
    for c in range(3):
        wait_part(weight, start_of(UP_WIDTHS, c), UP_WIDTHS[c], sems.at[c])

    def one(i, carry):
        fetch(i).wait()
        here = pl.ds(pl.multiple_of(i * 256, 256), 256)
        hidden = jnp.dot(normed[here, :], weight[...], preferred_element_type=F32)
        hidden = jnp.maximum(hidden, 0.0)
        squared_out[here, :] = (hidden * hidden).astype(BF)
        return carry

    lax.fori_loop(0, normed.shape[0] // 256, one, 0)


def down_kernel(places, targets, squared, *rest):
    partial_out, weight, sems = rest[6:]
    for c in range(3):
        at = start_of(DOWN_WIDTHS, c)
        place_half(places, targets, c, rest[2 * c : 2 * c + 2], weight, at, sems.at[c])
    for c in range(3):
        wait_part(weight, start_of(DOWN_WIDTHS, c), DOWN_WIDTHS[c], sems.at[c])

    def one(i, carry):
        here = pl.ds(pl.multiple_of(i * 256, 256), 256)
        partial_out[here, :] = nt_dot(squared[here, :], weight[...]).astype(BF)
        return carry

    lax.fori_loop(0, squared.shape[0] // 256, one, 0)


SMEM = pl.BlockSpec(memory_space=pltpu.SMEM)
VMEM = pl.BlockSpec(memory_space=pltpu.VMEM)
HBM = pl.BlockSpec(memory_space=pltpu.HBM)


def whole(shape):
    return pl.BlockSpec(shape, lambda i: (0,) * len(shape))


def rows_of(count, width):
    return pl.BlockSpec((count, width), lambda i: (i, 0))


def params(flops, nbytes, vmem_mib):
    return dict(
        compiler_params=pltpu.CompilerParams(vmem_limit_bytes=vmem_mib * 1024 * 1024),
        cost_estimate=pl.CostEstimate(flops=flops, bytes_accessed=nbytes, transcendentals=0),
    )


def on_device(
    tokens,
    attention_pre_gain,
    query_matrix,
    key_matrix,
    value_matrix,
    decay_first_weight,
    decay_second_weight,
    decay_offset_bias,
    extra_log_surge,
    readout_head_gain,
    output_matrix,
    attention_post_gain,
    feedforward_pre_gain,
    up_matrix,
    down_matrix,
    feedforward_post_gain,
):
    length = tokens.shape[0]
    rep, core = lax.axis_index("rep"), lax.axis_index("tp")
    fs = lax.axis_index(FS)
    mine_block = (fs * 2 + rep).astype(jnp.int32)
    core_in = core.astype(jnp.int32).reshape(1)
    table = jnp.asarray(OFFSETS)[core] ^ mine_block

    def half(shard):
        return lax.dynamic_slice_in_dim(shard, rep * HALF, HALF, axis=0)

    first = jnp.concatenate(
        [half(query_matrix), half(key_matrix), half(value_matrix), half(output_matrix.T)], axis=1
    )
    first = gather_start(first)
    up, down = half(up_matrix), half(down_matrix.T)
    feed = []
    for c in range(3):
        a, b = start_of(UP_WIDTHS, c), start_of(DOWN_WIDTHS, c)
        feed += [up[:, a : a + UP_WIDTHS[c]], down[:, b : b + DOWN_WIDTHS[c]]]
    feed = gather_start(jnp.concatenate(feed, axis=1))
    first_w, up_w, down_w = [], [], []
    lane = 0
    for c in range(3):
        held = columns(first, 512 * c, 512)
        for step in (3, 4):
            held = joined(held, over_link(held, step, c))
        first_w += [held, over_link(held, 5, c)]

        a, b = UP_WIDTHS[c], DOWN_WIDTHS[c]
        held = columns(feed, lane, a + b)
        lane += a + b
        held = joined(held, over_link(held, 3, c))
        pair = held, over_link(held, 4, c)
        held = columns(pair, 0, a)
        up_w += [held, over_link(held, 5, c)]
        held = columns(pair, a, b)
        down_w += [held, over_link(held, 5, c)]

    other = swap_cores(tokens)
    block = 256
    grid = (length // block,)
    normed, decay = pl.pallas_call(
        norm_kernel,
        grid=grid,
        in_specs=[
            SMEM,
            rows_of(block, 1024),
            rows_of(block, 1024),
            whole((1, 2048)),
            whole((2048, 16)),
            whole((16, 256)),
            whole((1, 256)),
            rows_of(block, 1),
        ],
        out_specs=[rows_of(block, 2048), rows_of(block, 256)],
        out_shape=[
            jax.ShapeDtypeStruct((length, 2048), BF),
            jax.ShapeDtypeStruct((length, 256), F32),
        ],
        name="norm",
        **params(400_000_000, 10_000_000, 16),
    )(
        core_in,
        tokens,
        other,
        attention_pre_gain.reshape(1, -1),
        decay_first_weight,
        decay_second_weight,
        decay_offset_bias.reshape(1, -1),
        extra_log_surge,
    )
    partial_attn = pl.pallas_call(
        attention_kernel,
        in_specs=[SMEM] + [VMEM] * 5 + [HBM] * 6,
        out_specs=VMEM,
        out_shape=jax.ShapeDtypeStruct((length, 2048), BF),
        scratch_shapes=[
            pltpu.VMEM((2048, 512), BF),
            pltpu.VMEM((2048, 512), BF),
            pltpu.VMEM((2048, 512), BF),
            pltpu.VMEM((512, 256), F32),
            pltpu.SemaphoreType.DMA((3,)),
        ],
        name="attention",
        **params(11_000_000_000, 14_000_000, 26),
    )(
        table,
        normed,
        decay,
        jnp.asarray(SMALL_LEVELS, BF),
        jnp.asarray(PAIR_LEVELS),
        readout_head_gain.reshape(1, -1),
        *first_w,
    )
    other_attn = swap_cores(partial_attn)
    other_gain = swap_cores(attention_post_gain)
    resid, normed_mid = pl.pallas_call(
        middle_kernel,
        grid=grid,
        in_specs=[
            SMEM,
            rows_of(block, 1024),
            rows_of(block, 1024),
            rows_of(block, 2048),
            rows_of(block, 2048),
            whole((1, 1024)),
            whole((1, 1024)),
            whole((1, 2048)),
        ],
        out_specs=[rows_of(block, 1024), rows_of(block, 2048)],
        out_shape=[
            jax.ShapeDtypeStruct((length, 1024), BF),
            pltpu.HBM((length, 2048), BF),
        ],
        name="middle",
        **params(60_000_000, 18_000_000, 20),
    )(
        core_in,
        tokens,
        other,
        partial_attn,
        other_attn,
        attention_post_gain.reshape(1, -1),
        other_gain.reshape(1, -1),
        feedforward_pre_gain.reshape(1, -1),
    )
    normed_mid = pltpu.with_memory_space_constraint(normed_mid, pltpu.HBM)
    squared = pl.pallas_call(
        up_kernel,
        in_specs=[SMEM] + [HBM] * 7,
        out_specs=VMEM,
        out_shape=jax.ShapeDtypeStruct((length, 2048), BF),
        scratch_shapes=[
            pltpu.VMEM((2048, 2048), BF),
            pltpu.VMEM((length, 2048), BF),
            pltpu.SemaphoreType.DMA((7,)),
        ],
        name="up_proj",
        **params(8_700_000_000, 16_000_000, 24),
    )(table, normed_mid, *up_w)

    def down_half(side):
        return pl.pallas_call(
            down_kernel,
            in_specs=[SMEM, SMEM, VMEM] + [HBM] * 6,
            out_specs=VMEM,
            out_shape=jax.ShapeDtypeStruct((length, 1024), BF),
            scratch_shapes=[pltpu.VMEM((1024, 2048), BF), pltpu.SemaphoreType.DMA((3,))],
            **params(4_300_000_000, 10_000_000, 20),
        )(
            jnp.asarray(HALF_PLACES)[core, side ^ (mine_block >> 5)],
            jnp.asarray(HALF_TARGETS)[core, side ^ (mine_block >> 5)] ^ (mine_block & 31),
            squared,
            *down_w,
        )

    away = down_half(1 - core)
    theirs = swap_cores(away)
    mine = down_half(core)
    feed = mine.astype(F32) + theirs.astype(F32)
    squares = jnp.sum(feed * feed, axis=1)
    squares_other = swap_cores(squares.reshape(8, 128)).reshape(length)
    scale = lax.rsqrt((squares + squares_other) / 2048 + EPS)[:, None]
    return (resid.astype(F32) + feed * scale * feedforward_post_gain).astype(BF)


def solution(mesh):
    finer = Mesh(
        mesh.devices.reshape(mesh.shape["rep"], 2, 4, 4, mesh.shape["tp"]),
        ("rep", "fs_0", "fs_1", "fs_2", "tp"),
    )
    in_specs = (
        P(REP_FS, "tp"),
        P(),
        P(FS, "tp"),
        P(FS, "tp"),
        P(FS, "tp"),
        P(),
        P(None, "tp"),
        P("tp"),
        P(REP_FS, "tp"),
        P(),
        P("tp", FS),
        P("tp"),
        P(),
        P(FS, "tp"),
        P("tp", FS),
        P("tp"),
    )

    return jax.shard_map(
        on_device, mesh=finer, in_specs=in_specs, out_specs=P(REP_FS, "tp"), check_vma=False
    )
```
